32 devices in a mesh: grp: 2 (over y), kv: 4 (over z), tp: 4 (over x, core).
Axes of the slice: x: 2, y: 2, z: 4, core: 2. Of those that a mesh axis runs over, the one named last changes fastest.
Arguments:
- stream: bfloat16 [256, 2048], P('grp', ('kv', 'tp')), parts along dimension 0, may hold values from -72 to 72
- lengths: int32 [256], P(('grp', 'kv')), parts along dimension 0, may hold values from 1 to 8, 384 in all
- delta_state: float32 [256, 32, 128, 128], P(('grp', 'kv'), 'tp'), parts along dimension 0, may hold values from -0.6 to 0.6
- q_hist: bfloat16 [256, 3, 2048], P(('grp', 'kv'), None, 'tp'), parts along dimension 0, may hold values from -6 to 6
- k_hist: bfloat16 [256, 3, 2048], P(('grp', 'kv'), None, 'tp'), parts along dimension 0, may hold values from -6 to 6
- v_hist: bfloat16 [256, 3, 4096], P(('grp', 'kv'), None, 'tp'), parts along dimension 0, may hold values from -6 to 6
- norm_gain: bfloat16 [2048], replicated, may hold values from 0.099609375 to 1.8984375
- w_query: bfloat16 [2048, 2048], P('kv', 'tp'), may hold values from -0.125 to 0.125
- w_key: bfloat16 [2048, 2048], P('kv', 'tp'), may hold values from -0.125 to 0.125
- w_value: bfloat16 [2048, 4096], P('kv', 'tp'), may hold values from -0.125 to 0.125
- w_gate: bfloat16 [2048, 4096], P('kv', 'tp'), may hold values from -0.125 to 0.125
- w_beta: bfloat16 [2048, 32], replicated, may hold values from -0.125 to 0.125
- w_decay: bfloat16 [2048, 32], replicated, may hold values from -0.125 to 0.125
- conv_query: bfloat16 [4, 2048], replicated, may hold values from -3 to 3
- conv_key: bfloat16 [4, 2048], replicated, may hold values from -3 to 3
- conv_value: bfloat16 [4, 4096], replicated, may hold values from -3 to 3
- decay_log: float32 [32], replicated, may hold values from 0 to 2.77
- time_bias: float32 [32], replicated, may hold values from -4 to 0
- out_gain: bfloat16 [128], replicated, may hold values from 0.099609375 to 1.8984375
- w_out: bfloat16 [4096, 2048], P('tp', 'kv'), may hold values from -0.09375 to 0.09375
- mlp_gain: bfloat16 [2048], replicated, may hold values from 0.099609375 to 1.8984375
- w_up: bfloat16 [2048, 8192], P('kv', 'tp'), may hold values from -0.125 to 0.125
- w_down: bfloat16 [8192, 2048], P('tp', 'kv'), may hold values from -0.0625 to 0.0625
Outputs:
- result: bfloat16 [256, 2048], P('grp', ('kv', 'tp')), parts along dimension 0
- new_state: float32 [256, 32, 128, 128], P(('grp', 'kv'), 'tp'), parts along dimension 0
The draws below stay inside these ranges and needn't reach their ends.
There are 2 independent parts, one for each index of `grp`. The reference program is written for one: setup_inputs(seed, part) draws one part's arguments, and reference() takes and returns one part's arrays. A program takes and returns all parts, laid end to end along the dimension named above; an argument that names none is the same for every part. Nothing has to cross between parts.
All inputs are finite; a program needn't handle non-finite values. No bound on the sum of `lengths` on one device may be relied on, other than what follows from the above.
Results may differ from the reference program's by a relative error of at most 0.01.
Values may be sent and summed in bfloat16 or wider, within the bound.
A program may use at most 128 MiB of HBM per device.

```python
import math
import jax
import jax.numpy as jnp
import numpy as np
from jax import lax

D = 2048
HEADS_K = 16
HEADS_V = 32
HEAD_DIM = 128
FF_UNITS = 8192
CONV = 4
SEQS = 128
N_KV = 4
N_TP = 4


def draw_stream(key, part):
    first_key, second_key, third_key = jax.random.split(jax.random.fold_in(key, 11), 3)
    columns = jnp.arange(D)
    block_number = columns // (D // N_KV)
    piece_number = columns // (D // (N_KV * N_TP)) % N_TP
    rising = 3.0 ** (block_number / max(N_KV - 1, 1)) * 3.0 ** (piece_number / max(N_TP - 1, 1))
    roughness = jax.random.uniform(first_key, (D,), jnp.float32, 0.5, 1.5)
    row_factor = jnp.exp(jax.random.uniform(second_key, (SEQS, 1), jnp.float32, 0.0, math.log(4.0)))
    base_values = jnp.clip(jax.random.normal(third_key, (SEQS, D), jnp.float32), -4.0, 4.0)
    return (base_values * rising * roughness * row_factor / 3.0).astype(jnp.bfloat16)


def block_scale(own_key, extent, cuts, smallest, largest):
    def one(dim, parts):
        steps = jax.random.uniform(jax.random.fold_in(jax.random.fold_in(own_key, 6), dim), (parts,), jnp.float32, smallest / len(cuts), largest / len(cuts))
        return jnp.repeat(jnp.exp(steps), extent[dim] // parts).reshape((-1,) + (1,) * (len(extent) - dim - 1))

    loudness = one(*cuts[0])
    for cut in cuts[1:]:
        loudness = loudness * one(*cut)
    return loudness


def profile(amount, total, reach, skew):
    portions = [(1 << 20) // math.isqrt(standing ** skew) + 1 for standing in range(2, amount + 1)]
    surplus, holding = total - reach - (amount - 1), [1] * (amount - 1)
    while surplus > 0:
        movable = [i for i in range(amount - 1) if holding[i] < reach]
        whole, remaining = sum([portions[i] for i in movable]), surplus
        for i in movable:
            extra = min(reach - holding[i], max(1, remaining * portions[i] // whole), surplus)
            holding[i] = holding[i] + extra
            surplus = surplus - extra
    return np.array([reach] + holding)


def uneven(rng, count, total, most, skew):
    if count == 2:
        one = jax.random.randint(rng, (), max(1, total - most), min(most, total - 1) + 1)
        return jnp.stack([one, total - one])
    sizes = jnp.asarray(profile(count, total, most, skew), jnp.int32)
    pairs = (count - 1) // 2
    donor, taker = sizes[1:1 + 2 * pairs:2], sizes[2:2 + 2 * pairs:2]
    room = jnp.minimum(donor - 1, most - taker)
    passed = jax.random.randint(jax.random.fold_in(rng, 1), (pairs,), 0, 1 << 20) % (room + 1)
    sizes = sizes.at[1:1 + 2 * pairs:2].set(donor - passed).at[2:2 + 2 * pairs:2].set(taker + passed)
    return sizes[jax.random.permutation(jax.random.fold_in(rng, 2), count)]


def normal_values(rng, extent, scale, most, cuts=(), held_as=jnp.bfloat16):
    drawn = scale * jax.random.normal(rng, extent, jnp.float32)
    if cuts:
        drawn = drawn * block_scale(rng, extent, cuts, -0.22, 0.18)
    return jnp.clip(drawn, -most, most).astype(held_as)


def setup_inputs(seed: int = 0, part: int = 0) -> dict:
    key_list = jax.random.split(jax.random.key(seed), 24)
    own_keys = jax.random.split(jax.random.fold_in(key_list[23], part), 24)
    stream = draw_stream(jax.random.fold_in(jax.random.fold_in(key_list[23], part), 71), part)
    lengths = uneven(own_keys[1], SEQS, 3 * SEQS, 8, 2).astype(jnp.int32)
    delta_state = normal_values(own_keys[2], (SEQS, HEADS_V, HEAD_DIM, HEAD_DIM), 0.1, 0.6, ((0, 4), (1, 4)), jnp.float32)
    q_hist = normal_values(own_keys[3], (SEQS, CONV - 1, HEADS_K * HEAD_DIM), 1.0, 6.0, ((0, 4), (2, 4)))
    k_hist = normal_values(own_keys[4], (SEQS, CONV - 1, HEADS_K * HEAD_DIM), 1.0, 6.0, ((0, 4), (2, 4)))
    v_hist = normal_values(own_keys[5], (SEQS, CONV - 1, HEADS_V * HEAD_DIM), 1.0, 6.0, ((0, 4), (2, 4)))
    norm_gain = jnp.clip(1.0 + 0.18 * jax.random.normal(key_list[6], (D,), jnp.float32), 0.099609375, 1.8984375).astype(jnp.bfloat16)
    w_query = normal_values(key_list[7], (D, HEADS_K * HEAD_DIM), D ** -0.5, 0.125, ((0, 4), (1, 4)))
    w_key = normal_values(key_list[8], (D, HEADS_K * HEAD_DIM), D ** -0.5, 0.125, ((0, 4), (1, 4)))
    w_value = normal_values(key_list[9], (D, HEADS_V * HEAD_DIM), D ** -0.5, 0.125, ((0, 4), (1, 4)))
    w_gate = normal_values(key_list[10], (D, HEADS_V * HEAD_DIM), D ** -0.5, 0.125, ((0, 4), (1, 4)))
    w_beta = normal_values(key_list[11], (D, HEADS_V), D ** -0.5, 0.125)
    w_decay = normal_values(key_list[12], (D, HEADS_V), D ** -0.5, 0.125)
    conv_query = normal_values(key_list[13], (CONV, HEADS_K * HEAD_DIM), CONV ** -0.5, 3.0)
    conv_key = normal_values(key_list[14], (CONV, HEADS_K * HEAD_DIM), CONV ** -0.5, 3.0)
    conv_value = normal_values(key_list[15], (CONV, HEADS_V * HEAD_DIM), CONV ** -0.5, 3.0)
    decay_log = jnp.clip(jax.random.uniform(key_list[16], (HEADS_V,), jnp.float32, 0.0, 2.77), 0.0, 2.77)
    time_bias = jnp.clip(jax.random.uniform(key_list[17], (HEADS_V,), jnp.float32, -4.0, 0.0), -4.0, 0.0)
    out_gain = jnp.clip(1.0 + 0.18 * jax.random.normal(key_list[18], (HEAD_DIM,), jnp.float32), 0.099609375, 1.8984375).astype(jnp.bfloat16)
    w_out = normal_values(key_list[19], (HEADS_V * HEAD_DIM, D), (HEADS_V * HEAD_DIM) ** -0.5, 0.09375, ((0, 4), (1, 4)))
    mlp_gain = jnp.clip(1.0 + 0.18 * jax.random.normal(key_list[20], (D,), jnp.float32), 0.099609375, 1.8984375).astype(jnp.bfloat16)
    w_up = normal_values(key_list[21], (D, FF_UNITS), D ** -0.5, 0.125, ((0, 4), (1, 4)))
    w_down = normal_values(key_list[22], (FF_UNITS, D), FF_UNITS ** -0.5, 0.0625, ((0, 4), (1, 4)))
    return {"stream": stream, "lengths": lengths, "delta_state": delta_state, "q_hist": q_hist, "k_hist": k_hist, "v_hist": v_hist, "norm_gain": norm_gain, "w_query": w_query, "w_key": w_key, "w_value": w_value, "w_gate": w_gate, "w_beta": w_beta, "w_decay": w_decay, "conv_query": conv_query, "conv_key": conv_key, "conv_value": conv_value, "decay_log": decay_log, "time_bias": time_bias, "out_gain": out_gain, "w_out": w_out, "mlp_gain": mlp_gain, "w_up": w_up, "w_down": w_down}


EPSILON = 1e-06

def unit_rows(values, factor):
    return values * lax.rsqrt(lax.optimization_barrier(jnp.sum(values * values, axis=-1, keepdims=True)) + EPSILON) * factor

def short_filter(current, history, weights, live_rows):
    history_live = jnp.where(live_rows[:, :, None], history.astype(jnp.float32), 0.0)
    filter_taps = weights.astype(jnp.float32)
    filtered = current * filter_taps[-1] + lax.optimization_barrier(jnp.sum(history_live * filter_taps[None, :-1], axis=1))
    return jax.nn.silu(filtered)

def delta_step(delta_state, fresh_rows, queries, keys_now, values_now, strength, log_fade):
    fade_factor = jnp.exp(log_fade)[:, :, None, None]
    carried = jnp.where(fresh_rows[:, None, None, None], 0.0, delta_state) * fade_factor
    recalled = lax.optimization_barrier(jnp.sum(carried * keys_now[:, :, :, None], axis=2))
    update = strength[:, :, None] * (values_now - recalled)
    new_state = carried + keys_now[:, :, :, None] * update[:, :, None, :]
    readout = lax.optimization_barrier(jnp.sum(new_state * queries[:, :, :, None], axis=2))
    return (new_state, readout)

def gated_norm(readout, gain, gate_in):
    normed = readout * lax.rsqrt(lax.optimization_barrier(jnp.mean(readout * readout, axis=-1, keepdims=True)) + EPSILON)
    return (normed * gain.astype(jnp.float32) * jax.nn.silu(gate_in)).astype(jnp.bfloat16)

def reference(stream, lengths, delta_state, q_hist, k_hist, v_hist, norm_gain, w_query, w_key, w_value, w_gate, w_beta, w_decay, conv_query, conv_key, conv_value, decay_log, time_bias, out_gain, w_out, mlp_gain, w_up, w_down):
    sequences = stream.shape[0]
    stream_wide = stream.astype(jnp.float32)
    row_scale = lax.rsqrt(lax.optimization_barrier(jnp.sum(stream_wide * stream_wide, axis=1, keepdims=True)) / D + EPSILON)
    scaled = (stream_wide * norm_gain.astype(jnp.float32)).astype(jnp.bfloat16)

    def project(weight):
        return jnp.dot(scaled, weight, preferred_element_type=jnp.float32) * row_scale
    live_rows = jnp.arange(CONV - 1, dtype=jnp.int32)[None, :] >= (CONV - lengths)[:, None]
    queries = short_filter(project(w_query), q_hist, conv_query, live_rows)
    keys_now = short_filter(project(w_key), k_hist, conv_key, live_rows)
    values_now = short_filter(project(w_value), v_hist, conv_value, live_rows)
    gate_in = project(w_gate).reshape(sequences, HEADS_V, HEAD_DIM)
    repeat_count = HEADS_V // HEADS_K
    queries = jnp.repeat(unit_rows(queries.reshape(sequences, HEADS_K, HEAD_DIM), HEAD_DIM ** (-0.5)), repeat_count, axis=1)
    keys_now = jnp.repeat(unit_rows(keys_now.reshape(sequences, HEADS_K, HEAD_DIM), 1.0), repeat_count, axis=1)
    values_now = values_now.reshape(sequences, HEADS_V, HEAD_DIM)
    strength = jax.nn.sigmoid(project(w_beta))
    log_fade = -jnp.exp(decay_log) * jax.nn.softplus(project(w_decay) + time_bias)
    new_state, readout = delta_step(delta_state, lengths == 1, queries, keys_now, values_now, strength, log_fade)
    gated = gated_norm(readout, out_gain, gate_in).reshape(sequences, HEADS_V * HEAD_DIM)
    mixed = (stream_wide + jnp.dot(gated, w_out, preferred_element_type=jnp.float32)).astype(jnp.bfloat16)
    mixed_wide = mixed.astype(jnp.float32)
    unit_scale = lax.rsqrt(lax.optimization_barrier(jnp.sum(mixed_wide * mixed_wide, axis=1, keepdims=True)) / D + EPSILON)
    scaled_mix = (mixed_wide * mlp_gain.astype(jnp.float32)).astype(jnp.bfloat16)
    unit_terms = jnp.dot(scaled_mix, w_up, preferred_element_type=jnp.float32) * unit_scale
    hidden = jnp.square(jax.nn.relu(unit_terms)).astype(jnp.bfloat16)
    result = (mixed_wide + jnp.dot(hidden, w_down, preferred_element_type=jnp.float32)).astype(jnp.bfloat16)
    return (result, new_state)
```

```python
import functools

import jax
import jax.numpy as jnp
from jax import lax
from jax.experimental import pallas as pl
from jax.experimental.pallas import tpu as pltpu
from jax.sharding import PartitionSpec as P

EPSILON = 1e-06
MESH = pl.DeviceIdType.MESH
F32 = jnp.float32
BF16 = jnp.bfloat16
LANES = 128
CONTRACT_LAST = (((1,), (1,)), ((), ()))


def greet(axes):
    barrier = pltpu.get_barrier_semaphore()
    total = 0
    for name, size in axes:
        me = lax.axis_index(name)
        for step in range(1, size):
            pl.semaphore_signal(
                barrier, inc=1, device_id={name: lax.rem(me + step, size)}, device_id_type=MESH
            )
            total += 1
    pl.semaphore_wait(barrier, total)


def order(size):
    return sorted(range(1, size), key=lambda step: -min(step, size - step))


def remote(name, peer, src, dst, send, recv):
    return pltpu.make_async_remote_copy(
        src_ref=src, dst_ref=dst, send_sem=send, recv_sem=recv,
        device_id={name: peer}, device_id_type=MESH,
    )


def scatter_copies(name, size, src, dst, send, recv):
    me = lax.axis_index(name)
    copies = []
    for step in order(size):
        peer = lax.rem(me + step, size)
        copies.append(
            remote(name, peer, src.at[peer], dst.at[step - 1], send.at[step - 1], recv.at[step - 1])
        )
    return copies


def gather_copies(name, size, src, dst, send, recv):
    me = lax.axis_index(name)
    copies = []
    for step in order(size):
        peer = lax.rem(me + step, size)
        copies.append(
            remote(name, peer, src, dst.at[me], send.at[step - 1], recv.at[step - 1])
        )
    return copies


def start(copies):
    for copy in copies:
        copy.start()


def wait_recv(copies):
    for copy in copies:
        copy.wait_recv()


def wait_send(copies):
    for copy in copies:
        copy.wait_send()


def unless(conditions, action):
    if not conditions:
        action()
        return
    skip = functools.reduce(jnp.logical_or, conditions)
    pl.when(jnp.logical_not(skip))(action)


class LineScatter:
    def __init__(self, name, size, part, got, relay_in, relay_out, send, recv, relay_recv):
        self.name, self.size, self.me = name, size, lax.axis_index(name)
        self.part, self.got = part, got
        self.relay_in, self.relay_out = relay_in, relay_out
        self.send, self.recv, self.relay_recv = send, recv, relay_recv
        self.relays = size >= 4

    def copy(self, c, step, src=None):
        peer = lax.rem(self.me + step, self.size)
        src = self.part.at[c, peer] if src is None else src
        return remote(
            self.name, peer, src, self.got.at[c, step - 1],
            self.send.at[c, step - 1], self.recv.at[c, step - 1],
        )

    def ends(self):
        last = self.size - 1
        return ((0, last, last, 1, last - 1), (last, 0, 1, last - 1, 2))

    def clear(self):
        if not self.relays:
            return
        for end, _, step, _, _ in self.ends():
            slot = self.size - step - 1

            @pl.when(self.me == end)
            def _():
                self.got[:, slot] = jnp.zeros(self.got.shape[:1] + self.got.shape[2:], self.got.dtype)

    def relay_copy(self, c, block, step, neighbour):
        return remote(
            self.name, neighbour, self.part.at[c, block], self.relay_in.at[c],
            self.send.at[c, step - 1], self.relay_recv.at[c],
        )

    def start(self, c):
        if self.relays:
            for end, block, step, neighbour, _ in self.ends():
                pl.when(self.me == end)(self.relay_copy(c, block, step, neighbour).start)
        for step in order(self.size):
            skips = []
            if self.relays:
                for end, _, far, neighbour, last in self.ends():
                    if step == far:
                        skips.append(self.me == end)
                    if step == last:
                        skips.append(self.me == neighbour)
            unless(skips, self.copy(c, step).start)

    def relay(self, c):
        if not self.relays:
            return
        for end, block, step, neighbour, last in self.ends():

            @pl.when(self.me == neighbour)
            def _():
                self.relay_copy(c, block, step, neighbour).wait_recv()
                total = self.relay_in[c].astype(F32) + self.part[c, block].astype(F32)
                self.relay_out[c] = total.astype(self.relay_out.dtype)
                self.copy(c, last, self.relay_out.at[c]).start()

    def total(self, c):
        for step in order(self.size):
            skips = []
            if self.relays:
                for end, _, far, _, _ in self.ends():
                    if step == self.size - far:
                        skips.append(self.me == end)
            unless(skips, self.copy(c, step).wait_recv)
        total = self.part[c, self.me].astype(F32)
        for slot in range(self.size - 1):
            total = total + self.got[c, slot].astype(F32)
        return total

    def finish(self, chunks):
        for c in range(chunks):
            for step in range(1, self.size):
                self.copy(c, step).wait_send()


class LineGather:
    def __init__(self, name, size, mine, everyone, send, recv, relay_send):
        self.name, self.size, self.me = name, size, lax.axis_index(name)
        self.mine, self.everyone = mine, everyone
        self.send, self.recv, self.relay_send = send, recv, relay_send
        self.relays = size >= 3

    def copy(self, c, step):
        peer = lax.rem(self.me + step, self.size)
        return remote(
            self.name, peer, self.mine.at[c], self.everyone.at[c, self.me],
            self.send.at[c, step - 1], self.recv.at[c, step - 1],
        )

    def skips(self, step):
        if not self.relays:
            return []
        skips = []
        if step != self.size - 1:
            skips.append(self.me == self.size - step)
        if step != 1:
            skips.append(self.me == self.size - 1 - step)
        return skips

    def start(self, c):
        for step in order(self.size):
            unless(self.skips(step), self.copy(c, step).start)

    def forwards(self):
        last = self.size - 1
        return ((1, 0, range(2, self.size)), (last - 1, last, range(last - 2, -1, -1)))

    def onward(self, c, end, source):
        step = (end - source) % self.size
        block = self.everyone.at[c, source]
        return remote(
            self.name, end, block, block, self.relay_send.at[c, source], self.recv.at[c, step - 1]
        )

    def forward(self, c):
        if not self.relays:
            return
        for neighbour, end, sources in self.forwards():

            @pl.when(self.me == neighbour)
            def _():
                for source in sources:
                    step = (neighbour - source) % self.size
                    self.copy(c, step).wait_recv()
                    self.onward(c, end, source).start()

    def wait(self, c):
        for step in order(self.size):
            skips = []
            if self.relays:
                if step != 1:
                    skips.append(self.me == 1)
                if step != self.size - 1:
                    skips.append(self.me == self.size - 2)
            unless(skips, self.copy(c, step).wait_recv)

    def finish(self, chunks):
        for c in range(chunks):
            for step in range(1, self.size):
                unless(self.skips(step), self.copy(c, step).wait_send)
            if self.relays:
                for neighbour, end, sources in self.forwards():

                    @pl.when(self.me == neighbour)
                    def _():
                        for source in sources:
                            self.onward(c, end, source).wait_send()


def silu(values):
    return values * jax.nn.sigmoid(values)


def softplus(values):
    return jnp.maximum(values, 0.0) + jnp.log1p(jnp.exp(-jnp.abs(values)))


def row_blocks(name, columns):
    return pl.ds(pl.multiple_of(lax.axis_index(name) * columns, LANES), columns)


def layer_kernel(
    n_kv, n_tp, width, head, repeat, chunks, pieces,
    stream, lengths, gain, decay_log, time_bias, out_gain, mlp_gain,
    w_b, w_d, w_q, w_k, w_v, w_g, q_hist, k_hist, v_hist, conv_q, conv_k, conv_v,
    w_out, w_up, w_down, state,
    result, new_state,
    stream_v, len_v, gain_v, dlog_v, bias_v, ogain_v, mgain_v,
    wb_v, wd_v, wq_v, wk_v, wv_v, wg_v, hist_q, hist_k, hist_v, convq_v, convk_v, convv_v,
    wo_v, wu_v, wdn_v,
    gains, params, streams, part_e, got_e,
    part_p, got_p, relay_pi, relay_po,
    key_s, query_s, value_s, fade_s, strength_s, dots_s, readouts,
    mine, gathered, mix_part, mix_got, mixed, blocks, sq_part, sq_got,
    up_part, up_got, relay_ui, relay_uo, hidden, hiddens, down_part, down_got,
    load_sem, state_sem, s_send, s_recv, e_send, e_recv,
    p_send, p_recv, p_relay, g_send, g_recv, g_relay,
    m_send, m_recv, b_send, b_recv, q_send, q_recv,
    u_send, u_recv, u_relay, h_send, h_recv, h_relay, d_send, d_recv,
):
    kv = lax.axis_index("kv")
    tp = lax.axis_index("tp")
    rows, own_cols = stream_v.shape
    own = rows // n_kv
    block = wq_v.shape[0]
    heads_all = w_b.shape[0]
    heads_own = chunks * repeat
    span = repeat * head
    block_cols = row_blocks("kv", block)

    sources = (
        (stream, stream_v),
        (gain, gain_v),
        (w_b.at[:, block_cols], wb_v), (w_d.at[:, block_cols], wd_v),
        (w_q, wq_v), (w_k, wk_v), (w_v, wv_v), (w_g, wg_v),
        (lengths, len_v), (decay_log, dlog_v), (time_bias, bias_v),
        (out_gain, ogain_v), (mlp_gain, mgain_v),
        (q_hist, hist_q), (k_hist, hist_k), (v_hist, hist_v),
        (conv_q.at[:, row_blocks("tp", convq_v.shape[1])], convq_v),
        (conv_k.at[:, row_blocks("tp", convk_v.shape[1])], convk_v),
        (conv_v.at[:, row_blocks("tp", convv_v.shape[1])], convv_v),
        (w_out, wo_v), (w_up, wu_v), (w_down, wdn_v),
    )
    loads = [pltpu.make_async_copy(src, dst, load_sem.at[i]) for i, (src, dst) in enumerate(sources)]
    state_loads = [
        pltpu.make_async_copy(
            state.at[:, c * repeat : (c + 1) * repeat],
            new_state.at[:, c * repeat : (c + 1) * repeat],
            state_sem.at[c],
        )
        for c in range(chunks)
    ]
    start(loads[:19])
    start(state_loads)
    start(loads[19:])

    scatter_p = LineScatter("kv", n_kv, part_p, got_p, relay_pi, relay_po, p_send, p_recv, p_relay)
    gather_g = LineGather("kv", n_kv, mine, gathered, g_send, g_recv, g_relay)
    scatter_u = LineScatter("kv", n_kv, up_part, up_got, relay_ui, relay_uo, u_send, u_recv, u_relay)
    gather_h = LineGather("kv", n_kv, hidden, hiddens, h_send, h_recv, h_relay)
    scatter_p.clear()
    scatter_u.clear()

    greet((("kv", n_kv), ("tp", n_tp)))
    loads[0].wait()
    stream_copies = gather_copies("tp", n_tp, stream_v, streams, s_send, s_recv)
    start(stream_copies)
    streams[tp] = stream_v[...]
    loads[1].wait()

    def gain_row(values):
        gains[...] = values[...].astype(F32)
        lines = block // LANES
        return jnp.concatenate(
            [gains[pl.ds(kv * lines + j, 1), :] for j in range(lines)], axis=1
        )

    norm_row = gain_row(gain_v)
    wait_recv(stream_copies)

    wide = jnp.concatenate([streams[t] for t in range(n_tp)], axis=1).astype(F32)
    scaled = (wide * norm_row).astype(BF16)
    squares = jnp.sum(wide * wide, axis=1, keepdims=True)
    loads[2].wait()
    loads[3].wait()
    beta = lax.dot_general(scaled, wb_v[...], CONTRACT_LAST, preferred_element_type=F32)
    decay = lax.dot_general(scaled, wd_v[...], CONTRACT_LAST, preferred_element_type=F32)
    part_e[...] = jnp.concatenate(
        [beta, decay, jnp.broadcast_to(squares, (rows, LANES - 2 * heads_all))], axis=1
    ).reshape(n_kv, own, LANES)
    extra_copies = scatter_copies("kv", n_kv, part_e, got_e, e_send, e_recv)
    start(extra_copies)

    for copy in loads[4:8]:
        copy.wait()
    fields = ((wq_v, head, 0), (wk_v, head, head), (wv_v, span, 2 * head), (wg_v, span, 2 * head + span))
    for c in range(chunks):
        for weight, size, offset in fields:
            product = jnp.dot(
                scaled, weight[:, c * size : (c + 1) * size], preferred_element_type=F32
            )
            part_p[c, :, :, offset : offset + size] = product.reshape(n_kv, own, size).astype(BF16)
        scatter_p.start(c)

    for copy in loads[8:19]:
        copy.wait()
    lens_row = jnp.broadcast_to(len_v[...].astype(F32), (own, own))
    diagonal = lax.broadcasted_iota(jnp.int32, (own, own), 0) == lax.broadcasted_iota(
        jnp.int32, (own, own), 1
    )
    length = jnp.sum(jnp.where(diagonal, lens_row, 0.0), axis=1, keepdims=True)

    def history(hist, taps):
        total = None
        count = taps.shape[0]
        for r in range(count - 1):
            live = length >= float(count - r)
            term = jnp.where(live, hist[r].astype(F32) * taps[r : r + 1, :], 0.0)
            total = term if total is None else total + term
        return total

    taps_q = convq_v[...].astype(F32)
    taps_k = convk_v[...].astype(F32)
    taps_v = convv_v[...].astype(F32)
    past_q = history(hist_q, taps_q)
    past_k = history(hist_k, taps_k)
    past_v = history(hist_v, taps_v)
    final = taps_q.shape[0] - 1

    params[...] = jnp.zeros(params.shape, F32)
    params[0:1, :heads_all] = dlog_v[...]
    params[1:2, :heads_all] = bias_v[...]
    shift = tp * heads_own
    own_params = pltpu.roll(params[...], lax.rem(LANES - shift, LANES), 1)

    wait_recv(extra_copies)
    extra = part_e[kv]
    for slot in range(n_kv - 1):
        extra = extra + got_e[slot]
    row_scale = lax.rsqrt(extra[:, 2 * heads_all : 2 * heads_all + 1] / width + EPSILON)
    terms = extra * row_scale
    own_beta = pltpu.roll(terms, lax.rem(LANES - shift, LANES), 1)
    own_decay = pltpu.roll(terms, lax.rem(2 * LANES - heads_all - shift, LANES), 1)
    fade = jnp.exp(-jnp.exp(own_params[0:1, :]) * softplus(own_decay + own_params[1:2, :]))
    fade = jnp.where(length == 1.0, 0.0, fade)
    strength = jax.nn.sigmoid(own_beta)
    gain_out = ogain_v[...].astype(F32)

    def unit(values, factor):
        return values * (
            lax.rsqrt(jnp.sum(values * values, axis=1, keepdims=True) + EPSILON) * factor
        )

    seqs = readouts.shape[1]

    def heads(c):
        total = scatter_p.total(c) * row_scale
        narrow = slice(c * head, (c + 1) * head)
        broad = slice(c * span, (c + 1) * span)
        query = unit(
            silu(total[:, :head] * taps_q[final : final + 1, narrow] + past_q[:, narrow]),
            head ** (-0.5),
        )
        key = unit(
            silu(total[:, head : 2 * head] * taps_k[final : final + 1, narrow] + past_k[:, narrow]),
            1.0,
        )
        query_s[...] = query
        key_s[...] = key
        value_s[...] = silu(
            total[:, 2 * head : 2 * head + span] * taps_v[final : final + 1, broad] + past_v[:, broad]
        )
        gate = silu(total[:, 2 * head + span :])
        dots_s[...] = jnp.broadcast_to(jnp.sum(query * key, axis=1, keepdims=True), (own, head))
        for j in range(repeat):
            v = c * repeat + j
            cols = slice(j * head, (j + 1) * head)
            fade_s[:, cols] = jnp.broadcast_to(fade[:, v : v + 1], (own, head))
            strength_s[:, cols] = jnp.broadcast_to(strength[:, v : v + 1], (own, head))
        state_loads[c].wait()

        @pl.loop(0, own // seqs)
        def _(g):
            base = g * seqs
            some = pl.ds(pl.multiple_of(base, seqs), seqs)
            keys_t = key_s[some, :].T
            queries_t = query_s[some, :].T
            dots = dots_s[some, :]
            values = value_s[some, :]
            fades = fade_s[some, :]
            strengths = strength_s[some, :]
            for s in range(seqs):
                key = jnp.broadcast_to(keys_t[:, s : s + 1], (head, head))
                query = jnp.broadcast_to(queries_t[:, s : s + 1], (head, head))
                line = slice(s, s + 1)
                for j in range(repeat):
                    cols = slice(j * head, (j + 1) * head)
                    held = new_state[base + s, c * repeat + j]
                    faded = fades[line, cols]
                    recalled = jnp.sum(held * key, axis=0, keepdims=True)
                    asked = jnp.sum(held * query, axis=0, keepdims=True)
                    update = strengths[line, cols] * (values[line, cols] - faded * recalled)
                    new_state[base + s, c * repeat + j] = held * faded + key * update
                    readouts[g, line, cols] = faded * asked + dots[line, :] * update

        for j in range(repeat):
            cols = slice(j * head, (j + 1) * head)
            one = readouts[:, :, cols].reshape(own, head)
            normed = one * lax.rsqrt(jnp.mean(one * one, axis=1, keepdims=True) + EPSILON)
            mine[c, :, cols] = (normed * gain_out * gate[:, cols]).astype(BF16)
        gather_g.start(c)
        gathered[c, kv] = mine[c]

    scatter_p.relay(0)
    for c in range(chunks):
        if c + 1 < chunks:
            scatter_p.relay(c + 1)
        heads(c)
        if c >= 1:
            gather_g.forward(c - 1)
    gather_g.forward(chunks - 1)

    def reduce_tp(product, part, got, send_sem, recv_sem):
        for t in range(n_tp):
            part[t] = product[:, t * own_cols : (t + 1) * own_cols].astype(BF16)
        copies = scatter_copies("tp", n_tp, part, got, send_sem, recv_sem)
        start(copies)
        wait_recv(copies)
        total = part[tp].astype(F32)
        for slot in range(n_tp - 1):
            total = total + got[slot].astype(F32)
        return total, copies

    loads[19].wait()
    product = jnp.zeros((rows, wo_v.shape[1]), F32)
    for c in range(chunks):
        gather_g.wait(c)
        product = product + jnp.dot(
            gathered[c].reshape(rows, span),
            wo_v[c * span : (c + 1) * span, :],
            preferred_element_type=F32,
        )
    total, mix_copies = reduce_tp(product, mix_part, mix_got, m_send, m_recv)
    mixed_own = (stream_v[...].astype(F32) + total).astype(BF16)
    mixed[...] = mixed_own
    block_copies = gather_copies("tp", n_tp, mixed, blocks, b_send, b_recv)
    start(block_copies)
    blocks[tp] = mixed_own
    mlp_row = gain_row(mgain_v)
    loads[20].wait()
    wait_recv(block_copies)
    wide = jnp.concatenate([blocks[t] for t in range(n_tp)], axis=1).astype(F32)
    scaled = (wide * mlp_row).astype(BF16)
    squares = jnp.sum(wide * wide, axis=1, keepdims=True)
    sq_part[...] = jnp.broadcast_to(squares, (rows, LANES)).reshape(n_kv, own, LANES)
    square_copies = scatter_copies("kv", n_kv, sq_part, sq_got, q_send, q_recv)
    start(square_copies)
    piece = wu_v.shape[1] // pieces
    for p in range(pieces):
        product = jnp.dot(
            scaled, wu_v[:, p * piece : (p + 1) * piece], preferred_element_type=F32
        )
        up_part[p] = product.reshape(n_kv, own, piece).astype(BF16)
        scatter_u.start(p)
    wait_recv(square_copies)
    square_sum = sq_part[kv]
    for slot in range(n_kv - 1):
        square_sum = square_sum + sq_got[slot]
    unit_scale = lax.rsqrt(square_sum[:, :1] / width + EPSILON)

    def activate(p):
        active = jnp.maximum(scatter_u.total(p) * unit_scale, 0.0)
        active = (active * active).astype(BF16)
        hidden[p] = active
        gather_h.start(p)
        hiddens[p, kv] = active

    scatter_u.relay(0)
    for p in range(pieces):
        if p + 1 < pieces:
            scatter_u.relay(p + 1)
        activate(p)
        if p >= 1:
            gather_h.forward(p - 1)
    gather_h.forward(pieces - 1)
    loads[21].wait()
    product = jnp.zeros((rows, wdn_v.shape[1]), F32)
    for p in range(pieces):
        gather_h.wait(p)
        product = product + jnp.dot(
            hiddens[p].reshape(rows, piece),
            wdn_v[p * piece : (p + 1) * piece, :],
            preferred_element_type=F32,
        )
    total, down_copies = reduce_tp(product, down_part, down_got, d_send, d_recv)
    result[...] = (mixed[...].astype(F32) + total).astype(BF16)
    for copies in (stream_copies, extra_copies, mix_copies, block_copies, square_copies, down_copies):
        wait_send(copies)
    scatter_p.finish(chunks)
    gather_g.finish(chunks)
    scatter_u.finish(pieces)
    gather_h.finish(pieces)


def on_device(
    n_kv, n_tp,
    stream, lengths, delta_state, q_hist, k_hist, v_hist, norm_gain,
    w_query, w_key, w_value, w_gate, w_beta, w_decay,
    conv_query, conv_key, conv_value, decay_log, time_bias, out_gain,
    w_out, mlp_gain, w_up, w_down,
):
    width = norm_gain.shape[0]
    rows, own_cols = stream.shape
    own, heads_own, head = delta_state.shape[:3]
    key_cols = q_hist.shape[2]
    value_cols = v_hist.shape[2]
    block = w_query.shape[0]
    heads_all = w_beta.shape[1]
    taps = conv_query.shape[0]
    chunks = key_cols // head
    repeat = heads_own // chunks
    span = repeat * head
    field = 2 * head + 2 * span
    units = w_up.shape[1]
    pieces = 4
    piece = units // pieces
    seqs = min(8, own)
    vmem = pl.BlockSpec(memory_space=pltpu.VMEM)
    hbm = pl.BlockSpec(memory_space=pltpu.HBM)
    dma = pltpu.SemaphoreType.DMA
    gain_shape = (width // LANES, LANES)
    ins = (
        stream, lengths[None], norm_gain.reshape(gain_shape), decay_log[None], time_bias[None],
        out_gain[None], mlp_gain.reshape(gain_shape),
        w_beta.T, w_decay.T, w_query, w_key, w_value, w_gate,
        *(jnp.transpose(hist, (1, 0, 2)) for hist in (q_hist, k_hist, v_hist)),
        conv_query, conv_key, conv_value, w_out, w_up, w_down, delta_state,
    )

    def buffer(*dims, dtype=BF16):
        return pltpu.VMEM(dims, dtype)

    result, new_state = pl.pallas_call(
        functools.partial(layer_kernel, n_kv, n_tp, width, head, repeat, chunks, pieces),
        out_shape=(
            pltpu.VMEM((rows, own_cols), BF16),
            pltpu.VMEM(delta_state.shape, F32),
        ),
        in_specs=[hbm] * len(ins),
        out_specs=(vmem, vmem),
        scratch_shapes=[
            buffer(rows, own_cols), buffer(1, own, dtype=jnp.int32), buffer(*gain_shape),
            buffer(1, heads_all, dtype=F32), buffer(1, heads_all, dtype=F32),
            buffer(1, head), buffer(*gain_shape),
            buffer(heads_all, block), buffer(heads_all, block),
            buffer(block, key_cols), buffer(block, key_cols),
            buffer(block, value_cols), buffer(block, value_cols),
            buffer(taps - 1, own, key_cols), buffer(taps - 1, own, key_cols),
            buffer(taps - 1, own, value_cols),
            buffer(taps, key_cols), buffer(taps, key_cols), buffer(taps, value_cols),
            buffer(*w_out.shape), buffer(*w_up.shape), buffer(*w_down.shape),
            buffer(*gain_shape, dtype=F32), buffer(8, LANES, dtype=F32),
            buffer(n_tp, rows, own_cols),
            buffer(n_kv, own, LANES, dtype=F32), buffer(n_kv - 1, own, LANES, dtype=F32),
            buffer(chunks, n_kv, own, field), buffer(chunks, n_kv - 1, own, field),
            buffer(chunks, own, field), buffer(chunks, own, field),
            buffer(own, head, dtype=F32), buffer(own, head, dtype=F32),
            buffer(own, span, dtype=F32), buffer(own, span, dtype=F32),
            buffer(own, span, dtype=F32), buffer(own, head, dtype=F32),
            buffer(own // seqs, seqs, span, dtype=F32),
            buffer(chunks, own, span), buffer(chunks, n_kv, own, span),
            buffer(n_tp, rows, own_cols), buffer(n_tp - 1, rows, own_cols),
            buffer(rows, own_cols), buffer(n_tp, rows, own_cols),
            buffer(n_kv, own, LANES, dtype=F32), buffer(n_kv - 1, own, LANES, dtype=F32),
            buffer(pieces, n_kv, own, piece), buffer(pieces, n_kv - 1, own, piece),
            buffer(pieces, own, piece), buffer(pieces, own, piece),
            buffer(pieces, own, piece), buffer(pieces, n_kv, own, piece),
            buffer(n_tp, rows, own_cols), buffer(n_tp - 1, rows, own_cols),
            dma((22,)), dma((chunks,)),
            dma((n_tp - 1,)), dma((n_tp - 1,)),
            dma((n_kv - 1,)), dma((n_kv - 1,)),
            dma((chunks, n_kv - 1)), dma((chunks, n_kv - 1)), dma((chunks,)),
            dma((chunks, n_kv - 1)), dma((chunks, n_kv - 1)), dma((chunks, n_kv)),
            dma((n_tp - 1,)), dma((n_tp - 1,)),
            dma((n_tp - 1,)), dma((n_tp - 1,)),
            dma((n_kv - 1,)), dma((n_kv - 1,)),
            dma((pieces, n_kv - 1)), dma((pieces, n_kv - 1)), dma((pieces,)),
            dma((pieces, n_kv - 1)), dma((pieces, n_kv - 1)), dma((pieces, n_kv)),
            dma((n_tp - 1,)), dma((n_tp - 1,)),
        ],
        compiler_params=pltpu.CompilerParams(
            collective_id=0, has_side_effects=True,
            vmem_limit_bytes=67043328 - delta_state.size * 4 - 2**18,
        ),
        name="layer",
    )(*ins)
    return result, new_state


def solution(mesh):
    in_specs = (
        P("grp", ("kv", "tp")),
        P(("grp", "kv")),
        P(("grp", "kv"), "tp", None, None),
        P(("grp", "kv"), None, "tp"),
        P(("grp", "kv"), None, "tp"),
        P(("grp", "kv"), None, "tp"),
        P(),
        P("kv", "tp"),
        P("kv", "tp"),
        P("kv", "tp"),
        P("kv", "tp"),
        P(),
        P(),
        P(),
        P(),
        P(),
        P(),
        P(),
        P(),
        P("tp", "kv"),
        P(),
        P("kv", "tp"),
        P("tp", "kv"),
    )
    out_specs = (P("grp", ("kv", "tp")), P(("grp", "kv"), "tp", None, None))
    return jax.shard_map(
        functools.partial(on_device, mesh.shape["kv"], mesh.shape["tp"]),
        mesh=mesh, in_specs=in_specs, out_specs=out_specs, check_vma=False,
    )
```

```python
import functools

import jax
import jax.numpy as jnp
from jax import lax
from jax.experimental import pallas as pl
from jax.experimental.pallas import tpu as pltpu
from jax.sharding import PartitionSpec as P

EPSILON = 1e-06
MESH = pl.DeviceIdType.MESH
F32 = jnp.float32
BF16 = jnp.bfloat16
LANES = 128
LEAD = 1
DIRECT_LAST = 1
CONTRACT_LAST = (((1,), (1,)), ((), ()))


def greet(axes):
    barrier = pltpu.get_barrier_semaphore()
    total = 0
    for name, size in axes:
        me = lax.axis_index(name)
        for step in range(1, size):
            pl.semaphore_signal(
                barrier, inc=1, device_id={name: lax.rem(me + step, size)}, device_id_type=MESH
            )
            total += 1
    pl.semaphore_wait(barrier, total)


def order(size):
    return sorted(range(1, size), key=lambda step: -min(step, size - step))


def remote(name, peer, src, dst, send, recv):
    return pltpu.make_async_remote_copy(
        src_ref=src, dst_ref=dst, send_sem=send, recv_sem=recv,
        device_id={name: peer}, device_id_type=MESH,
    )


def scatter_copies(name, size, src, dst, send, recv):
    me = lax.axis_index(name)
    copies = []
    for step in order(size):
        peer = lax.rem(me + step, size)
        copies.append(
            remote(name, peer, src.at[peer], dst.at[step - 1], send.at[step - 1], recv.at[step - 1])
        )
    return copies


def gather_copies(name, size, src, dst, send, recv):
    me = lax.axis_index(name)
    copies = []
    for step in order(size):
        peer = lax.rem(me + step, size)
        copies.append(
            remote(name, peer, src, dst.at[me], send.at[step - 1], recv.at[step - 1])
        )
    return copies


def start(copies):
    for copy in copies:
        copy.start()


def wait_recv(copies):
    for copy in copies:
        copy.wait_recv()


def wait_send(copies):
    for copy in copies:
        copy.wait_send()


def unless(conditions, action):
    if not conditions:
        action()
        return
    skip = functools.reduce(jnp.logical_or, conditions)
    pl.when(jnp.logical_not(skip))(action)


class LineScatter:
    def __init__(self, name, size, part, got, relay_in, relay_out, send, recv, relay_recv):
        self.name, self.size, self.me = name, size, lax.axis_index(name)
        self.part, self.got = part, got
        self.relay_in, self.relay_out = relay_in, relay_out
        self.send, self.recv, self.relay_recv = send, recv, relay_recv
        self.chunks = part.shape[0]
        self.relays = size >= 4

    def copy(self, c, step, src=None):
        peer = lax.rem(self.me + step, self.size)
        src = self.part.at[c, peer] if src is None else src
        return remote(
            self.name, peer, src, self.got.at[c, step - 1],
            self.send.at[c, step - 1], self.recv.at[c, step - 1],
        )

    def ends(self):
        last = self.size - 1
        return ((0, last, last, 1, last - 1), (last, 0, 1, last - 1, 2))

    def clear(self):
        if not self.relays:
            return
        for end, _, step, _, _ in self.ends():
            slot = self.size - step - 1

            @pl.when(self.me == end)
            def _():
                self.got[:, slot] = jnp.zeros(self.got.shape[:1] + self.got.shape[2:], self.got.dtype)

    def relay_copy(self, c, block, step, neighbour):
        return remote(
            self.name, neighbour, self.part.at[c, block], self.relay_in.at[c],
            self.send.at[c, step - 1], self.relay_recv.at[c],
        )

    def start(self, c):
        if self.relays:
            for end, block, step, neighbour, _ in self.ends():
                pl.when(self.me == end)(self.relay_copy(c, block, step, neighbour).start)
        for step in order(self.size):
            skips = []
            if self.relays:
                for end, _, far, neighbour, last in self.ends():
                    if step == far:
                        skips.append(self.me == end)
                    if step == last or c >= LEAD:
                        skips.append(self.me == neighbour)
            unless(skips, self.copy(c, step).start)

    def relay(self, c):
        if not self.relays:
            return
        for end, block, step, neighbour, last in self.ends():

            @pl.when(self.me == neighbour)
            def _():
                self.relay_copy(c, block, step, neighbour).wait_recv()
                total = self.relay_in[c].astype(F32) + self.part[c, block].astype(F32)
                self.relay_out[c] = total.astype(self.relay_out.dtype)
                self.copy(c, last, self.relay_out.at[c]).start()
                if c + LEAD < self.chunks:
                    for hop in order(self.size):
                        if hop != last:
                            self.copy(c + LEAD, hop).start()

    def total(self, c):
        for step in order(self.size):
            skips = []
            if self.relays:
                for end, _, far, _, _ in self.ends():
                    if step == self.size - far:
                        skips.append(self.me == end)
            unless(skips, self.copy(c, step).wait_recv)
        total = self.part[c, self.me].astype(F32)
        for slot in range(self.size - 1):
            total = total + self.got[c, slot].astype(F32)
        return total

    def finish(self, chunks):
        for c in range(chunks):
            for step in range(1, self.size):
                self.copy(c, step).wait_send()


class LineGather:
    def __init__(self, name, size, mine, everyone, send, recv, relay_send):
        self.name, self.size, self.me = name, size, lax.axis_index(name)
        self.mine, self.everyone = mine, everyone
        self.send, self.recv, self.relay_send = send, recv, relay_send
        self.relays = size >= 3
        self.direct = () if DIRECT_LAST == 0 else range(mine.shape[0] - DIRECT_LAST, mine.shape[0])

    def copy(self, c, step):
        peer = lax.rem(self.me + step, self.size)
        return remote(
            self.name, peer, self.mine.at[c], self.everyone.at[c, self.me],
            self.send.at[c, step - 1], self.recv.at[c, step - 1],
        )

    def skips(self, c, step):
        if not self.relays or c in self.direct:
            return []
        skips = []
        if step != self.size - 1:
            skips.append(self.me == self.size - step)
        if step != 1:
            skips.append(self.me == self.size - 1 - step)
        return skips

    def start(self, c):
        for step in order(self.size):
            unless(self.skips(c, step), self.copy(c, step).start)

    def forwards(self):
        last = self.size - 1
        return ((1, 0, range(2, self.size)), (last - 1, last, range(last - 2, -1, -1)))

    def onward(self, c, end, source):
        step = (end - source) % self.size
        block = self.everyone.at[c, source]
        return remote(
            self.name, end, block, block, self.relay_send.at[c, source], self.recv.at[c, step - 1]
        )

    def forward(self, c):
        if not self.relays or c in self.direct:
            return
        for neighbour, end, sources in self.forwards():

            @pl.when(self.me == neighbour)
            def _():
                for source in sources:
                    step = (neighbour - source) % self.size
                    self.copy(c, step).wait_recv()
                    self.onward(c, end, source).start()

    def wait(self, c):
        for step in order(self.size):
            skips = []
            if self.relays and c not in self.direct:
                if step != 1:
                    skips.append(self.me == 1)
                if step != self.size - 1:
                    skips.append(self.me == self.size - 2)
            unless(skips, self.copy(c, step).wait_recv)

    def finish(self, chunks):
        for c in range(chunks):
            for step in range(1, self.size):
                unless(self.skips(c, step), self.copy(c, step).wait_send)
            if self.relays and c not in self.direct:
                for neighbour, end, sources in self.forwards():

                    @pl.when(self.me == neighbour)
                    def _():
                        for source in sources:
                            self.onward(c, end, source).wait_send()


def silu(values):
    return values * jax.nn.sigmoid(values)


def softplus(values):
    return jnp.maximum(values, 0.0) + jnp.log1p(jnp.exp(-jnp.abs(values)))


def row_blocks(name, columns):
    return pl.ds(pl.multiple_of(lax.axis_index(name) * columns, LANES), columns)


def layer_kernel(
    n_kv, n_tp, width, head, repeat, chunks, pieces,
    stream, lengths, gain, decay_log, time_bias, out_gain, mlp_gain,
    w_b, w_d, w_q, w_k, w_v, w_g, q_hist, k_hist, v_hist, conv_q, conv_k, conv_v,
    w_out, w_up, w_down, state,
    result, new_state,
    stream_v, len_v, gain_v, dlog_v, bias_v, ogain_v, mgain_v,
    wb_v, wd_v, wq_v, wk_v, wv_v, wg_v, hist_q, hist_k, hist_v, convq_v, convk_v, convv_v,
    wo_v, wu_v, wdn_v,
    gains, params, streams, part_e, got_e,
    part_p, got_p, relay_pi, relay_po,
    readouts,
    mine, gathered, mix_part, mix_got, mixed, blocks, sq_part, sq_got,
    up_part, up_got, relay_ui, relay_uo, hidden, hiddens, down_part, down_got,
    load_sem, state_sem, s_send, s_recv, e_send, e_recv,
    p_send, p_recv, p_relay, g_send, g_recv, g_relay,
    m_send, m_recv, b_send, b_recv, q_send, q_recv,
    u_send, u_recv, u_relay, h_send, h_recv, h_relay, d_send, d_recv,
):
    kv = lax.axis_index("kv")
    tp = lax.axis_index("tp")
    rows, own_cols = stream_v.shape
    own = rows // n_kv
    block = wq_v.shape[0]
    heads_all = w_b.shape[0]
    heads_own = chunks * repeat
    span = repeat * head
    block_cols = row_blocks("kv", block)

    sources = (
        (stream, stream_v),
        (gain, gain_v),
        (w_b.at[:, block_cols], wb_v), (w_d.at[:, block_cols], wd_v),
        (w_q, wq_v), (w_k, wk_v), (w_v, wv_v), (w_g, wg_v),
        (lengths, len_v), (decay_log, dlog_v), (time_bias, bias_v),
        (out_gain, ogain_v), (mlp_gain, mgain_v),
        (q_hist, hist_q), (k_hist, hist_k), (v_hist, hist_v),
        (conv_q.at[:, row_blocks("tp", convq_v.shape[1])], convq_v),
        (conv_k.at[:, row_blocks("tp", convk_v.shape[1])], convk_v),
        (conv_v.at[:, row_blocks("tp", convv_v.shape[1])], convv_v),
        (w_out, wo_v), (w_up, wu_v), (w_down, wdn_v),
    )
    loads = [pltpu.make_async_copy(src, dst, load_sem.at[i]) for i, (src, dst) in enumerate(sources)]
    state_loads = [
        pltpu.make_async_copy(
            state.at[:, c * repeat : (c + 1) * repeat],
            new_state.at[:, c * repeat : (c + 1) * repeat],
            state_sem.at[c],
        )
        for c in range(chunks)
    ]
    start(loads[:19])
    start(state_loads)
    start(loads[19:])

    scatter_p = LineScatter("kv", n_kv, part_p, got_p, relay_pi, relay_po, p_send, p_recv, p_relay)
    gather_g = LineGather("kv", n_kv, mine, gathered, g_send, g_recv, g_relay)
    scatter_u = LineScatter("kv", n_kv, up_part, up_got, relay_ui, relay_uo, u_send, u_recv, u_relay)
    gather_h = LineGather("kv", n_kv, hidden, hiddens, h_send, h_recv, h_relay)
    scatter_p.clear()
    scatter_u.clear()

    greet((("kv", n_kv), ("tp", n_tp)))
    loads[0].wait()
    stream_copies = gather_copies("tp", n_tp, stream_v, streams, s_send, s_recv)
    start(stream_copies)
    streams[tp] = stream_v[...]
    loads[1].wait()

    def gain_row(values):
        gains[...] = values[...].astype(F32)
        lines = block // LANES
        return jnp.concatenate(
            [gains[pl.ds(kv * lines + j, 1), :] for j in range(lines)], axis=1
        )

    norm_row = gain_row(gain_v)
    wait_recv(stream_copies)

    wide = jnp.concatenate([streams[t] for t in range(n_tp)], axis=1).astype(F32)
    scaled = (wide * norm_row).astype(BF16)
    squares = jnp.sum(wide * wide, axis=1, keepdims=True)
    loads[2].wait()
    loads[3].wait()
    beta = lax.dot_general(scaled, wb_v[...], CONTRACT_LAST, preferred_element_type=F32)
    decay = lax.dot_general(scaled, wd_v[...], CONTRACT_LAST, preferred_element_type=F32)
    part_e[...] = jnp.concatenate(
        [beta, decay, jnp.broadcast_to(squares, (rows, LANES - 2 * heads_all))], axis=1
    ).reshape(n_kv, own, LANES)
    extra_copies = scatter_copies("kv", n_kv, part_e, got_e, e_send, e_recv)
    start(extra_copies)

    for copy in loads[4:8]:
        copy.wait()
    fields = ((wq_v, head, 0), (wk_v, head, head), (wv_v, span, 2 * head), (wg_v, span, 2 * head + span))
    for c in range(chunks):
        for weight, size, offset in fields:
            product = jnp.dot(
                scaled, weight[:, c * size : (c + 1) * size], preferred_element_type=F32
            )
            part_p[c, :, :, offset : offset + size] = product.reshape(n_kv, own, size).astype(BF16)
        scatter_p.start(c)

    for copy in loads[8:19]:
        copy.wait()
    lens_row = jnp.broadcast_to(len_v[...].astype(F32), (own, own))
    diagonal = lax.broadcasted_iota(jnp.int32, (own, own), 0) == lax.broadcasted_iota(
        jnp.int32, (own, own), 1
    )
    length = jnp.sum(jnp.where(diagonal, lens_row, 0.0), axis=1, keepdims=True)

    def history(hist, taps):
        total = None
        count = taps.shape[0]
        for r in range(count - 1):
            live = length >= float(count - r)
            term = jnp.where(live, hist[r].astype(F32) * taps[r : r + 1, :], 0.0)
            total = term if total is None else total + term
        return total

    taps_q = convq_v[...].astype(F32)
    taps_k = convk_v[...].astype(F32)
    taps_v = convv_v[...].astype(F32)
    past_q = history(hist_q, taps_q)
    past_k = history(hist_k, taps_k)
    past_v = history(hist_v, taps_v)
    final = taps_q.shape[0] - 1

    params[...] = jnp.zeros(params.shape, F32)
    params[0:1, :heads_all] = dlog_v[...]
    params[1:2, :heads_all] = bias_v[...]
    shift = tp * heads_own
    own_params = pltpu.roll(params[...], lax.rem(LANES - shift, LANES), 1)

    wait_recv(extra_copies)
    extra = part_e[kv]
    for slot in range(n_kv - 1):
        extra = extra + got_e[slot]
    row_scale = lax.rsqrt(extra[:, 2 * heads_all : 2 * heads_all + 1] / width + EPSILON)
    terms = extra * row_scale
    own_beta = pltpu.roll(terms, lax.rem(LANES - shift, LANES), 1)
    own_decay = pltpu.roll(terms, lax.rem(2 * LANES - heads_all - shift, LANES), 1)
    fade = jnp.exp(-jnp.exp(own_params[0:1, :]) * softplus(own_decay + own_params[1:2, :]))
    fade = jnp.where(length == 1.0, 0.0, fade)
    strength = jax.nn.sigmoid(own_beta)
    gain_out = ogain_v[...].astype(F32)

    def unit(values, factor):
        return values * (
            lax.rsqrt(jnp.sum(values * values, axis=1, keepdims=True) + EPSILON) * factor
        )

    seqs = readouts.shape[1]

    def heads(c):
        total = scatter_p.total(c) * row_scale
        narrow = slice(c * head, (c + 1) * head)
        broad = slice(c * span, (c + 1) * span)
        query = unit(
            silu(total[:, :head] * taps_q[final : final + 1, narrow] + past_q[:, narrow]),
            head ** (-0.5),
        )
        key = unit(
            silu(total[:, head : 2 * head] * taps_k[final : final + 1, narrow] + past_k[:, narrow]),
            1.0,
        )
        values = silu(
            total[:, 2 * head : 2 * head + span] * taps_v[final : final + 1, broad] + past_v[:, broad]
        )
        gate = silu(total[:, 2 * head + span :])
        dot = jnp.sum(query * key, axis=1, keepdims=True)
        owned = range(c * repeat, (c + 1) * repeat)

        def widen(columns):
            return jnp.concatenate(
                [jnp.broadcast_to(column, (own, head)) for column in columns], axis=1
            )

        dots = widen([dot] * repeat)
        fades = widen([fade[:, v : v + 1] for v in owned])
        strengths = widen([strength[:, v : v + 1] for v in owned])
        keys_t = key.T
        line = lax.broadcasted_iota(jnp.int32, (seqs, span), 0)
        state_loads[c].wait()

        def ask(g):
            some = slice(g * seqs, (g + 1) * seqs)
            both = jnp.concatenate([key[some], query[some]], axis=0).astype(BF16)
            recalled = jnp.zeros((seqs, span), F32)
            asked = jnp.zeros((seqs, span), F32)
            for s in range(seqs):
                held = jnp.concatenate([new_state[g * seqs + s, v] for v in owned], axis=1)
                answer = jnp.dot(both, held.astype(BF16), preferred_element_type=F32)
                recalled = jnp.where(line == s, answer[:seqs], recalled)
                asked = jnp.where(line == s, answer[seqs:], asked)
            faded = fades[some]
            update = strengths[some] * (values[some] - faded * recalled)
            readouts[g] = faded * asked + dots[some] * update
            return faded, update

        def apply(g, faded, update):
            for s in range(seqs):
                q = g * seqs + s
                wide_key = jnp.broadcast_to(keys_t[:, q : q + 1], (head, head))
                for j, v in enumerate(owned):
                    cols = slice(j * head, (j + 1) * head)
                    new_state[q, v] = (
                        new_state[q, v] * faded[s : s + 1, cols] + wide_key * update[s : s + 1, cols]
                    )

        groups = own // seqs
        ready = ask(0)
        for g in range(groups):
            later = ask(g + 1) if g + 1 < groups else None
            apply(g, *ready)
            ready = later

        for j in range(repeat):
            cols = slice(j * head, (j + 1) * head)
            one = readouts[:, :, cols].reshape(own, head)
            normed = one * lax.rsqrt(jnp.mean(one * one, axis=1, keepdims=True) + EPSILON)
            mine[c, :, cols] = (normed * gain_out * gate[:, cols]).astype(BF16)
        gather_g.start(c)
        gathered[c, kv] = mine[c]

    scatter_p.relay(0)
    for c in range(chunks):
        if c + 1 < chunks:
            scatter_p.relay(c + 1)
        heads(c)
        if c == chunks - 2:
            gather_g.forward(0)
    for c in range(1 if chunks > 1 else 0, chunks):
        gather_g.forward(c)

    def reduce_tp(product, part, got, send_sem, recv_sem, meanwhile=None):
        for t in range(n_tp):
            part[t] = product[:, t * own_cols : (t + 1) * own_cols].astype(BF16)
        copies = scatter_copies("tp", n_tp, part, got, send_sem, recv_sem)
        start(copies)
        if meanwhile is not None:
            meanwhile()
        wait_recv(copies)
        total = part[tp].astype(F32)
        for slot in range(n_tp - 1):
            total = total + got[slot].astype(F32)
        return total, copies

    loads[19].wait()
    product = jnp.zeros((rows, wo_v.shape[1]), F32)
    for c in range(chunks):
        gather_g.wait(c)
        product = product + jnp.dot(
            gathered[c].reshape(rows, span),
            wo_v[c * span : (c + 1) * span, :],
            preferred_element_type=F32,
        )
    total, mix_copies = reduce_tp(product, mix_part, mix_got, m_send, m_recv)
    mixed_own = (stream_v[...].astype(F32) + total).astype(BF16)
    mixed[...] = mixed_own
    block_copies = gather_copies("tp", n_tp, mixed, blocks, b_send, b_recv)
    start(block_copies)
    blocks[tp] = mixed_own
    mlp_row = gain_row(mgain_v)
    loads[20].wait()
    wait_recv(block_copies)
    wide = jnp.concatenate([blocks[t] for t in range(n_tp)], axis=1).astype(F32)
    scaled = (wide * mlp_row).astype(BF16)
    piece = wu_v.shape[1] // pieces
    for p in range(pieces):
        product = jnp.dot(
            scaled, wu_v[:, p * piece : (p + 1) * piece], preferred_element_type=F32
        )
        up_part[p] = product.reshape(n_kv, own, piece).astype(BF16)
        scatter_u.start(p)
    corner = lax.broadcasted_iota(jnp.int32, (rows, rows), 0) == lax.broadcasted_iota(
        jnp.int32, (rows, rows), 1
    )
    squares = jnp.sum(wide * wide, axis=1, keepdims=True)
    flat = jnp.sum(jnp.where(corner, squares, 0.0), axis=0, keepdims=True)
    sq_part[...] = jnp.broadcast_to(flat, sq_part.shape)
    square_copies = gather_copies("kv", n_kv, sq_part, sq_got, q_send, q_recv)
    start(square_copies)
    sq_got[kv] = sq_part[...]
    scatter_p.finish(chunks)
    gather_g.finish(chunks)

    def activate(p):
        active = jnp.maximum(scatter_u.total(p), 0.0)
        active = (active * active).astype(BF16)
        hidden[p] = active
        gather_h.start(p)
        hiddens[p, kv] = active

    scatter_u.relay(0)
    for p in range(pieces):
        if p + 1 < pieces:
            scatter_u.relay(p + 1)
        activate(p)
    for p in range(pieces):
        gather_h.forward(p)
    loads[21].wait()
    wait_recv(square_copies)
    square_sum = sq_got[0]
    for z in range(1, n_kv):
        square_sum = square_sum + sq_got[z]
    spread = jnp.broadcast_to(1.0 / (square_sum[0:1, :] / width + EPSILON), (rows, rows))
    scale_squared = jnp.sum(jnp.where(corner, spread, 0.0), axis=1, keepdims=True)
    product = jnp.zeros((rows, wdn_v.shape[1]), F32)
    for p in range(pieces):
        gather_h.wait(p)
        product = product + jnp.dot(
            hiddens[p].reshape(rows, piece),
            wdn_v[p * piece : (p + 1) * piece, :],
            preferred_element_type=F32,
        )

    def settle():
        for copies in (stream_copies, extra_copies, mix_copies, block_copies, square_copies):
            wait_send(copies)
        scatter_u.finish(pieces)
        gather_h.finish(pieces)

    total, down_copies = reduce_tp(
        product * scale_squared, down_part, down_got, d_send, d_recv, settle
    )
    result[...] = (mixed[...].astype(F32) + total).astype(BF16)
    wait_send(down_copies)


def on_device(
    n_kv, n_tp,
    stream, lengths, delta_state, q_hist, k_hist, v_hist, norm_gain,
    w_query, w_key, w_value, w_gate, w_beta, w_decay,
    conv_query, conv_key, conv_value, decay_log, time_bias, out_gain,
    w_out, mlp_gain, w_up, w_down,
):
    width = norm_gain.shape[0]
    rows, own_cols = stream.shape
    own, heads_own, head = delta_state.shape[:3]
    key_cols = q_hist.shape[2]
    value_cols = v_hist.shape[2]
    block = w_query.shape[0]
    heads_all = w_beta.shape[1]
    taps = conv_query.shape[0]
    chunks = key_cols // head
    repeat = heads_own // chunks
    span = repeat * head
    field = 2 * head + 2 * span
    units = w_up.shape[1]
    pieces = 4
    piece = units // pieces
    seqs = min(8, own)
    vmem = pl.BlockSpec(memory_space=pltpu.VMEM)
    hbm = pl.BlockSpec(memory_space=pltpu.HBM)
    dma = pltpu.SemaphoreType.DMA
    gain_shape = (width // LANES, LANES)
    ins = (
        stream, lengths[None], norm_gain.reshape(gain_shape), decay_log[None], time_bias[None],
        out_gain[None], mlp_gain.reshape(gain_shape),
        w_beta.T, w_decay.T, w_query, w_key, w_value, w_gate,
        *(jnp.transpose(hist, (1, 0, 2)) for hist in (q_hist, k_hist, v_hist)),
        conv_query, conv_key, conv_value, w_out, w_up, w_down, delta_state,
    )

    def buffer(*dims, dtype=BF16):
        return pltpu.VMEM(dims, dtype)

    result, new_state = pl.pallas_call(
        functools.partial(layer_kernel, n_kv, n_tp, width, head, repeat, chunks, pieces),
        out_shape=(
            pltpu.VMEM((rows, own_cols), BF16),
            pltpu.VMEM(delta_state.shape, F32),
        ),
        in_specs=[hbm] * len(ins),
        out_specs=(vmem, vmem),
        scratch_shapes=[
            buffer(rows, own_cols), buffer(1, own, dtype=jnp.int32), buffer(*gain_shape),
            buffer(1, heads_all, dtype=F32), buffer(1, heads_all, dtype=F32),
            buffer(1, head), buffer(*gain_shape),
            buffer(heads_all, block), buffer(heads_all, block),
            buffer(block, key_cols), buffer(block, key_cols),
            buffer(block, value_cols), buffer(block, value_cols),
            buffer(taps - 1, own, key_cols), buffer(taps - 1, own, key_cols),
            buffer(taps - 1, own, value_cols),
            buffer(taps, key_cols), buffer(taps, key_cols), buffer(taps, value_cols),
            buffer(*w_out.shape), buffer(*w_up.shape), buffer(*w_down.shape),
            buffer(*gain_shape, dtype=F32), buffer(8, LANES, dtype=F32),
            buffer(n_tp, rows, own_cols),
            buffer(n_kv, own, LANES, dtype=F32), buffer(n_kv - 1, own, LANES, dtype=F32),
            buffer(chunks, n_kv, own, field), buffer(chunks, n_kv - 1, own, field),
            buffer(chunks, own, field), buffer(chunks, own, field),
            buffer(own // seqs, seqs, span, dtype=F32),
            buffer(chunks, own, span), buffer(chunks, n_kv, own, span),
            buffer(n_tp, rows, own_cols), buffer(n_tp - 1, rows, own_cols),
            buffer(rows, own_cols), buffer(n_tp, rows, own_cols),
            buffer(8, rows, dtype=F32), buffer(n_kv, 8, rows, dtype=F32),
            buffer(pieces, n_kv, own, piece), buffer(pieces, n_kv - 1, own, piece),
            buffer(pieces, own, piece), buffer(pieces, own, piece),
            buffer(pieces, own, piece), buffer(pieces, n_kv, own, piece),
            buffer(n_tp, rows, own_cols), buffer(n_tp - 1, rows, own_cols),
            dma((22,)), dma((chunks,)),
            dma((n_tp - 1,)), dma((n_tp - 1,)),
            dma((n_kv - 1,)), dma((n_kv - 1,)),
            dma((chunks, n_kv - 1)), dma((chunks, n_kv - 1)), dma((chunks,)),
            dma((chunks, n_kv - 1)), dma((chunks, n_kv - 1)), dma((chunks, n_kv)),
            dma((n_tp - 1,)), dma((n_tp - 1,)),
            dma((n_tp - 1,)), dma((n_tp - 1,)),
            dma((n_kv - 1,)), dma((n_kv - 1,)),
            dma((pieces, n_kv - 1)), dma((pieces, n_kv - 1)), dma((pieces,)),
            dma((pieces, n_kv - 1)), dma((pieces, n_kv - 1)), dma((pieces, n_kv)),
            dma((n_tp - 1,)), dma((n_tp - 1,)),
        ],
        compiler_params=pltpu.CompilerParams(
            collective_id=0, has_side_effects=True,
            vmem_limit_bytes=67043328 - delta_state.size * 4 - 2**18,
        ),
        name="layer",
    )(*ins)
    return result, new_state


def solution(mesh):
    in_specs = (
        P("grp", ("kv", "tp")),
        P(("grp", "kv")),
        P(("grp", "kv"), "tp", None, None),
        P(("grp", "kv"), None, "tp"),
        P(("grp", "kv"), None, "tp"),
        P(("grp", "kv"), None, "tp"),
        P(),
        P("kv", "tp"),
        P("kv", "tp"),
        P("kv", "tp"),
        P("kv", "tp"),
        P(),
        P(),
        P(),
        P(),
        P(),
        P(),
        P(),
        P(),
        P("tp", "kv"),
        P(),
        P("kv", "tp"),
        P("tp", "kv"),
    )
    out_specs = (P("grp", ("kv", "tp")), P(("grp", "kv"), "tp", None, None))
    return jax.shard_map(
        functools.partial(on_device, mesh.shape["kv"], mesh.shape["tp"]),
        mesh=mesh, in_specs=in_specs, out_specs=out_specs, check_vma=False,
    )
```

```python
import functools

import jax
import jax.numpy as jnp
from jax import lax
from jax.experimental import pallas as pl
from jax.experimental.pallas import tpu as pltpu
from jax.sharding import PartitionSpec as P

EPSILON = 1e-06
MESH = pl.DeviceIdType.MESH
F32 = jnp.float32
BF16 = jnp.bfloat16
LANES = 128
LEAD = 2
DIRECT_LAST = 1
CONTRACT_LAST = (((1,), (1,)), ((), ()))


def greet(axes):
    barrier = pltpu.get_barrier_semaphore()
    total = 0
    for name, size in axes:
        me = lax.axis_index(name)
        for step in range(1, size):
            pl.semaphore_signal(
                barrier, inc=1, device_id={name: lax.rem(me + step, size)}, device_id_type=MESH
            )
            total += 1
    pl.semaphore_wait(barrier, total)


def order(size):
    return sorted(range(1, size), key=lambda step: -min(step, size - step))


def remote(name, peer, src, dst, send, recv):
    return pltpu.make_async_remote_copy(
        src_ref=src, dst_ref=dst, send_sem=send, recv_sem=recv,
        device_id={name: peer}, device_id_type=MESH,
    )


def scatter_copies(name, size, src, dst, send, recv):
    me = lax.axis_index(name)
    copies = []
    for step in order(size):
        peer = lax.rem(me + step, size)
        copies.append(
            remote(name, peer, src.at[peer], dst.at[step - 1], send.at[step - 1], recv.at[step - 1])
        )
    return copies


def gather_copies(name, size, src, dst, send, recv):
    me = lax.axis_index(name)
    copies = []
    for step in order(size):
        peer = lax.rem(me + step, size)
        copies.append(
            remote(name, peer, src, dst.at[me], send.at[step - 1], recv.at[step - 1])
        )
    return copies


def start(copies):
    for copy in copies:
        copy.start()


def wait_recv(copies):
    for copy in copies:
        copy.wait_recv()


def wait_send(copies):
    for copy in copies:
        copy.wait_send()


def unless(conditions, action):
    if not conditions:
        action()
        return
    skip = functools.reduce(jnp.logical_or, conditions)
    pl.when(jnp.logical_not(skip))(action)


class LineScatter:
    def __init__(
        self, name, size, group, part, got, relay_in, relay_out, send, recv, relay_recv
    ):
        self.name, self.size, self.me = name, size, lax.axis_index(name)
        self.part, self.got = part, got
        self.relay_in, self.relay_out = relay_in, relay_out
        self.send, self.recv, self.relay_recv = send, recv, relay_recv
        self.chunks, self.group = part.shape[0], group
        self.relays = size >= 4

    def copy(self, c, step, src=None):
        peer = lax.rem(self.me + step, self.size)
        src = self.part.at[c, peer] if src is None else src
        return remote(
            self.name, peer, src, self.got.at[c, step - 1],
            self.send.at[c, step - 1], self.recv.at[c, step - 1],
        )

    def ends(self):
        last = self.size - 1
        return ((0, last, last, 1, last - 1), (last, 0, 1, last - 1, 2))

    def clear(self):
        if not self.relays:
            return
        for end, _, step, _, _ in self.ends():
            slot = self.size - step - 1

            @pl.when(self.me == end)
            def _():
                self.got[:, slot] = jnp.zeros(self.got.shape[:1] + self.got.shape[2:], self.got.dtype)

    def relay_copy(self, c, block, step, neighbour):
        return remote(
            self.name, neighbour, self.part.at[c, block], self.relay_in.at[c],
            self.send.at[c, step - 1], self.relay_recv.at[c],
        )

    def start(self, c):
        if self.relays:
            for end, block, step, neighbour, _ in self.ends():
                pl.when(self.me == end)(self.relay_copy(c, block, step, neighbour).start)
        for step in order(self.size):
            skips = []
            if self.relays:
                for end, _, far, neighbour, last in self.ends():
                    if step == far:
                        skips.append(self.me == end)
                    if step == last or c % self.group >= LEAD:
                        skips.append(self.me == neighbour)
            unless(skips, self.copy(c, step).start)

    def relay(self, c):
        if not self.relays:
            return
        for end, block, step, neighbour, last in self.ends():

            @pl.when(self.me == neighbour)
            def _():
                self.relay_copy(c, block, step, neighbour).wait_recv()
                total = self.relay_in[c].astype(F32) + self.part[c, block].astype(F32)
                self.relay_out[c] = total.astype(self.relay_out.dtype)
                self.copy(c, last, self.relay_out.at[c]).start()
                if c + LEAD < self.chunks and (c + LEAD) % self.group >= LEAD:
                    for hop in order(self.size):
                        if hop != last:
                            self.copy(c + LEAD, hop).start()

    def total(self, c):
        for step in order(self.size):
            skips = []
            if self.relays:
                for end, _, far, _, _ in self.ends():
                    if step == self.size - far:
                        skips.append(self.me == end)
            unless(skips, self.copy(c, step).wait_recv)
        total = self.part[c, self.me].astype(F32)
        for slot in range(self.size - 1):
            total = total + self.got[c, slot].astype(F32)
        return total

    def finish(self, chunks):
        for c in range(chunks):
            for step in range(1, self.size):
                self.copy(c, step).wait_send()


class LineGather:
    def __init__(self, name, size, group, mine, everyone, send, recv, relay_send):
        self.name, self.size, self.me = name, size, lax.axis_index(name)
        self.mine, self.everyone = mine, everyone
        self.send, self.recv, self.relay_send = send, recv, relay_send
        self.relays = size >= 3
        self.direct = [c for c in range(mine.shape[0]) if c % group >= group - DIRECT_LAST]

    def copy(self, c, step):
        peer = lax.rem(self.me + step, self.size)
        return remote(
            self.name, peer, self.mine.at[c], self.everyone.at[c, self.me],
            self.send.at[c, step - 1], self.recv.at[c, step - 1],
        )

    def skips(self, c, step):
        if not self.relays or c in self.direct:
            return []
        skips = []
        if step != self.size - 1:
            skips.append(self.me == self.size - step)
        if step != 1:
            skips.append(self.me == self.size - 1 - step)
        return skips

    def start(self, c):
        for step in order(self.size):
            unless(self.skips(c, step), self.copy(c, step).start)

    def forwards(self):
        last = self.size - 1
        return ((1, 0, range(2, self.size)), (last - 1, last, range(last - 2, -1, -1)))

    def onward(self, c, end, source):
        step = (end - source) % self.size
        block = self.everyone.at[c, source]
        return remote(
            self.name, end, block, block, self.relay_send.at[c, source], self.recv.at[c, step - 1]
        )

    def forward(self, c):
        if not self.relays or c in self.direct:
            return
        for neighbour, end, sources in self.forwards():

            @pl.when(self.me == neighbour)
            def _():
                for source in sources:
                    step = (neighbour - source) % self.size
                    self.copy(c, step).wait_recv()
                    self.onward(c, end, source).start()

    def wait(self, c):
        for step in order(self.size):
            skips = []
            if self.relays and c not in self.direct:
                if step != 1:
                    skips.append(self.me == 1)
                if step != self.size - 1:
                    skips.append(self.me == self.size - 2)
            unless(skips, self.copy(c, step).wait_recv)

    def finish(self, chunks):
        for c in range(chunks):
            for step in range(1, self.size):
                unless(self.skips(c, step), self.copy(c, step).wait_send)
            if self.relays and c not in self.direct:
                for neighbour, end, sources in self.forwards():

                    @pl.when(self.me == neighbour)
                    def _():
                        for source in sources:
                            self.onward(c, end, source).wait_send()


def silu(values):
    return values * jax.nn.sigmoid(values)


def softplus(values):
    return jnp.maximum(values, 0.0) + jnp.log1p(jnp.exp(-jnp.abs(values)))


def row_blocks(name, columns):
    return pl.ds(pl.multiple_of(lax.axis_index(name) * columns, LANES), columns)


def layer_kernel(
    n_kv, n_tp, width, head, repeat, chunks, pieces, halves,
    stream, lengths, gain, decay_log, time_bias, out_gain, mlp_gain,
    w_b, w_d, w_q, w_k, w_v, w_g, q_hist, k_hist, v_hist, conv_q, conv_k, conv_v,
    w_out, w_up, w_down, state,
    result, new_state,
    stream_v, len_v, gain_v, dlog_v, bias_v, ogain_v, mgain_v,
    wb_v, wd_v, wq_v, wk_v, wv_v, wg_v, hist_q, hist_k, hist_v, convq_v, convk_v, convv_v,
    wo_v, wu_v, wdn_v,
    gains, params, streams, part_e, got_e,
    part_p, got_p, relay_pi, relay_po,
    readouts,
    mine, gathered, mix_part, mix_got, mixed, blocks, sq_part, sq_got,
    up_part, up_got, relay_ui, relay_uo, hidden, hiddens, down_part, down_got,
    load_sem, state_sem, s_send, s_recv, e_send, e_recv,
    p_send, p_recv, p_relay, g_send, g_recv, g_relay,
    m_send, m_recv, b_send, b_recv, q_send, q_recv,
    u_send, u_recv, u_relay, h_send, h_recv, h_relay, d_send, d_recv,
):
    kv = lax.axis_index("kv")
    tp = lax.axis_index("tp")
    rows, own_cols = stream_v.shape
    own = rows // n_kv
    share = own // halves
    half_rows = n_kv * share
    block = wq_v.shape[0]
    heads_all = w_b.shape[0]
    heads_own = chunks * repeat
    span = repeat * head
    block_cols = row_blocks("kv", block)

    sources = (
        (stream, stream_v),
        (gain, gain_v),
        (w_b.at[:, block_cols], wb_v), (w_d.at[:, block_cols], wd_v),
        (w_q, wq_v), (w_k, wk_v), (w_v, wv_v), (w_g, wg_v),
        (lengths, len_v), (decay_log, dlog_v), (time_bias, bias_v),
        (out_gain, ogain_v), (mlp_gain, mgain_v),
        (q_hist, hist_q), (k_hist, hist_k), (v_hist, hist_v),
        (conv_q.at[:, row_blocks("tp", convq_v.shape[1])], convq_v),
        (conv_k.at[:, row_blocks("tp", convk_v.shape[1])], convk_v),
        (conv_v.at[:, row_blocks("tp", convv_v.shape[1])], convv_v),
        (w_out, wo_v), (w_up, wu_v), (w_down, wdn_v),
    )
    loads = [pltpu.make_async_copy(src, dst, load_sem.at[i]) for i, (src, dst) in enumerate(sources)]
    state_loads = [
        pltpu.make_async_copy(
            state.at[:, c * repeat : (c + 1) * repeat],
            new_state.at[:, c * repeat : (c + 1) * repeat],
            state_sem.at[c],
        )
        for c in range(chunks)
    ]
    start(loads[:19])
    start(state_loads)
    start(loads[19:])

    scatter_p = LineScatter("kv", n_kv, halves * chunks, part_p, got_p, relay_pi, relay_po, p_send, p_recv, p_relay)
    gather_g = LineGather("kv", n_kv, chunks, mine, gathered, g_send, g_recv, g_relay)
    scatter_u = LineScatter("kv", n_kv, pieces, up_part, up_got, relay_ui, relay_uo, u_send, u_recv, u_relay)
    gather_h = LineGather("kv", n_kv, pieces, hidden, hiddens, h_send, h_recv, h_relay)
    scatter_p.clear()
    scatter_u.clear()

    greet((("kv", n_kv), ("tp", n_tp)))
    loads[0].wait()
    stream_copies = gather_copies("tp", n_tp, stream_v, streams, s_send, s_recv)
    start(stream_copies)
    streams[tp] = stream_v[...]
    loads[1].wait()

    def gain_row(values):
        gains[...] = values[...].astype(F32)
        lines = block // LANES
        return jnp.concatenate(
            [gains[pl.ds(kv * lines + j, 1), :] for j in range(lines)], axis=1
        )

    norm_row = gain_row(gain_v)
    wait_recv(stream_copies)

    wide = jnp.concatenate([streams[t] for t in range(n_tp)], axis=1).astype(F32)
    scaled = (wide * norm_row).astype(BF16)
    squares = jnp.sum(wide * wide, axis=1, keepdims=True)
    loads[2].wait()
    loads[3].wait()
    beta = lax.dot_general(scaled, wb_v[...], CONTRACT_LAST, preferred_element_type=F32)
    decay = lax.dot_general(scaled, wd_v[...], CONTRACT_LAST, preferred_element_type=F32)
    part_e[...] = jnp.concatenate(
        [beta, decay, jnp.broadcast_to(squares, (rows, LANES - 2 * heads_all))], axis=1
    ).reshape(n_kv, own, LANES)
    extra_copies = scatter_copies("kv", n_kv, part_e, got_e, e_send, e_recv)
    start(extra_copies)

    for copy in loads[4:8]:
        copy.wait()
    fields = ((wq_v, head, 0), (wk_v, head, head), (wv_v, span, 2 * head), (wg_v, span, 2 * head + span))
    for c in range(chunks):
        for weight, size, offset in fields:
            product = jnp.dot(
                scaled, weight[:, c * size : (c + 1) * size], preferred_element_type=F32
            )
            split = product.reshape(n_kv, own, size).astype(BF16)
            for h in range(halves):
                part_p[h * chunks + c, :, :, offset : offset + size] = split[
                    :, h * share : (h + 1) * share
                ]
        scatter_p.start(c)

    for copy in loads[8:19]:
        copy.wait()
    lens_row = jnp.broadcast_to(len_v[...].astype(F32), (own, own))
    diagonal = lax.broadcasted_iota(jnp.int32, (own, own), 0) == lax.broadcasted_iota(
        jnp.int32, (own, own), 1
    )
    length = jnp.sum(jnp.where(diagonal, lens_row, 0.0), axis=1, keepdims=True)

    def history(hist, taps):
        total = None
        count = taps.shape[0]
        for r in range(count - 1):
            live = length >= float(count - r)
            term = jnp.where(live, hist[r].astype(F32) * taps[r : r + 1, :], 0.0)
            total = term if total is None else total + term
        return total

    taps_q = convq_v[...].astype(F32)
    taps_k = convk_v[...].astype(F32)
    taps_v = convv_v[...].astype(F32)
    past_q = history(hist_q, taps_q)
    past_k = history(hist_k, taps_k)
    past_v = history(hist_v, taps_v)
    final = taps_q.shape[0] - 1

    params[...] = jnp.zeros(params.shape, F32)
    params[0:1, :heads_all] = dlog_v[...]
    params[1:2, :heads_all] = bias_v[...]
    shift = tp * heads_own
    own_params = pltpu.roll(params[...], lax.rem(LANES - shift, LANES), 1)

    wait_recv(extra_copies)
    extra = part_e[kv]
    for slot in range(n_kv - 1):
        extra = extra + got_e[slot]
    row_scale = lax.rsqrt(extra[:, 2 * heads_all : 2 * heads_all + 1] / width + EPSILON)
    terms = extra * row_scale
    own_beta = pltpu.roll(terms, lax.rem(LANES - shift, LANES), 1)
    own_decay = pltpu.roll(terms, lax.rem(2 * LANES - heads_all - shift, LANES), 1)
    fade = jnp.exp(-jnp.exp(own_params[0:1, :]) * softplus(own_decay + own_params[1:2, :]))
    fade = jnp.where(length == 1.0, 0.0, fade)
    strength = jax.nn.sigmoid(own_beta)
    gain_out = ogain_v[...].astype(F32)

    def unit(values, factor):
        return values * (
            lax.rsqrt(jnp.sum(values * values, axis=1, keepdims=True) + EPSILON) * factor
        )

    seqs = readouts.shape[1]

    def heads(h, c):
        index = h * chunks + c
        these = slice(h * share, (h + 1) * share)
        total = scatter_p.total(index) * row_scale[these]
        narrow = slice(c * head, (c + 1) * head)
        broad = slice(c * span, (c + 1) * span)
        query = unit(
            silu(total[:, :head] * taps_q[final : final + 1, narrow] + past_q[these, narrow]),
            head ** (-0.5),
        )
        key = unit(
            silu(total[:, head : 2 * head] * taps_k[final : final + 1, narrow] + past_k[these, narrow]),
            1.0,
        )
        values = silu(
            total[:, 2 * head : 2 * head + span] * taps_v[final : final + 1, broad] + past_v[these, broad]
        )
        gate = silu(total[:, 2 * head + span :])
        dot = jnp.sum(query * key, axis=1, keepdims=True)
        owned = range(c * repeat, (c + 1) * repeat)

        def widen(columns):
            return jnp.concatenate(
                [jnp.broadcast_to(column, (share, head)) for column in columns], axis=1
            )

        dots = widen([dot] * repeat)
        fades = widen([fade[these, v : v + 1] for v in owned])
        strengths = widen([strength[these, v : v + 1] for v in owned])
        keys_t = key.T
        line = lax.broadcasted_iota(jnp.int32, (seqs, span), 0)
        if h == 0:
            state_loads[c].wait()

        def ask(g):
            some = slice(g * seqs, (g + 1) * seqs)
            both = jnp.concatenate([key[some], query[some]], axis=0).astype(BF16)
            recalled = jnp.zeros((seqs, span), F32)
            asked = jnp.zeros((seqs, span), F32)
            for s in range(seqs):
                q = h * share + g * seqs + s
                held = jnp.concatenate([new_state[q, v] for v in owned], axis=1)
                answer = jnp.dot(both, held.astype(BF16), preferred_element_type=F32)
                recalled = jnp.where(line == s, answer[:seqs], recalled)
                asked = jnp.where(line == s, answer[seqs:], asked)
            faded = fades[some]
            update = strengths[some] * (values[some] - faded * recalled)
            readouts[g] = faded * asked + dots[some] * update
            return faded, update

        def apply(g, faded, update):
            for s in range(seqs):
                q = h * share + g * seqs + s
                near = g * seqs + s
                wide_key = jnp.broadcast_to(keys_t[:, near : near + 1], (head, head))
                for j, v in enumerate(owned):
                    cols = slice(j * head, (j + 1) * head)
                    new_state[q, v] = (
                        new_state[q, v] * faded[s : s + 1, cols] + wide_key * update[s : s + 1, cols]
                    )

        groups = share // seqs
        ready = ask(0)
        for g in range(groups):
            later = ask(g + 1) if g + 1 < groups else None
            apply(g, *ready)
            ready = later

        for j in range(repeat):
            cols = slice(j * head, (j + 1) * head)
            one = readouts[:, :, cols].reshape(share, head)
            normed = one * lax.rsqrt(jnp.mean(one * one, axis=1, keepdims=True) + EPSILON)
            mine[index, :, cols] = (normed * gain_out * gate[:, cols]).astype(BF16)
        gather_g.start(index)
        gathered[index, kv] = mine[index]

    def project_relay(h, c):
        scatter_p.relay(h * chunks + c)

    def project_start(h, c):
        scatter_p.start(h * chunks + c)

    def gated_forward(h, c):
        gather_g.forward(h * chunks + c)

    copies_of = {}

    def send_tp(name, h, product, part, got, send_sem, recv_sem):
        for t in range(n_tp):
            part[h, t] = product[:, t * own_cols : (t + 1) * own_cols].astype(BF16)
        copies = scatter_copies("tp", n_tp, part.at[h], got.at[h], send_sem.at[h], recv_sem.at[h])
        start(copies)
        copies_of[name, h] = copies

    def sum_tp(name, h, part, got):
        wait_recv(copies_of[name, h])
        total = part[h, tp].astype(F32)
        for slot in range(n_tp - 1):
            total = total + got[h, slot].astype(F32)
        return total

    def out_project(h):
        if h == 0:
            loads[19].wait()
        product = jnp.zeros((half_rows, wo_v.shape[1]), F32)
        for c in range(chunks):
            gather_g.wait(h * chunks + c)
            product = product + jnp.dot(
                gathered[h * chunks + c].reshape(half_rows, span),
                wo_v[c * span : (c + 1) * span, :],
                preferred_element_type=F32,
            )
        send_tp("mix", h, product, mix_part, mix_got, m_send, m_recv)

    def mix(h):
        total = sum_tp("mix", h, mix_part, mix_got)
        before = jnp.concatenate(
            [stream_v[z * own + h * share : z * own + (h + 1) * share, :] for z in range(n_kv)], axis=0
        )
        mixed_own = (before.astype(F32) + total).astype(BF16)
        mixed[h] = mixed_own
        copies = gather_copies("tp", n_tp, mixed.at[h], blocks.at[h], b_send.at[h], b_recv.at[h])
        start(copies)
        copies_of["block", h] = copies
        blocks[h, tp] = mixed_own

    mlp_row = gain_row(mgain_v)
    piece = wu_v.shape[1] // pieces
    corner = lax.broadcasted_iota(jnp.int32, (half_rows, half_rows), 0) == lax.broadcasted_iota(
        jnp.int32, (half_rows, half_rows), 1
    )

    def up(h):
        if h == 0:
            loads[20].wait()
        wait_recv(copies_of["block", h])
        wide = jnp.concatenate([blocks[h, t] for t in range(n_tp)], axis=1).astype(F32)
        scaled = (wide * mlp_row).astype(BF16)
        for p in range(pieces):
            product = jnp.dot(
                scaled, wu_v[:, p * piece : (p + 1) * piece], preferred_element_type=F32
            )
            up_part[h * pieces + p] = product.reshape(n_kv, share, piece).astype(BF16)
            scatter_u.start(h * pieces + p)
        squares = jnp.sum(wide * wide, axis=1, keepdims=True)
        flat = jnp.sum(jnp.where(corner, squares, 0.0), axis=0, keepdims=True)
        sq_part[h, :, :half_rows] = jnp.broadcast_to(flat, (sq_part.shape[1], half_rows))
        copies = gather_copies("kv", n_kv, sq_part.at[h], sq_got.at[h], q_send.at[h], q_recv.at[h])
        start(copies)
        copies_of["square", h] = copies
        sq_got[h, kv, :, :half_rows] = sq_part[h, :, :half_rows]

    def up_relay(h, p):
        scatter_u.relay(h * pieces + p)

    def activate(h, p):
        index = h * pieces + p
        active = jnp.maximum(scatter_u.total(index), 0.0)
        active = (active * active).astype(BF16)
        hidden[index] = active
        gather_h.start(index)
        hiddens[index, kv] = active

    def hidden_forward(h, p):
        gather_h.forward(h * pieces + p)

    def down(h):
        if h == 0:
            loads[21].wait()
        wait_recv(copies_of["square", h])
        square_sum = sq_got[h, 0, :, :half_rows]
        for z in range(1, n_kv):
            square_sum = square_sum + sq_got[h, z, :, :half_rows]
        spread = jnp.broadcast_to(
            1.0 / (square_sum[0:1, :] / width + EPSILON), (half_rows, half_rows)
        )
        scale_squared = jnp.sum(jnp.where(corner, spread, 0.0), axis=1, keepdims=True)
        product = jnp.zeros((half_rows, wdn_v.shape[1]), F32)
        for p in range(pieces):
            index = h * pieces + p
            gather_h.wait(index)
            product = product + jnp.dot(
                hiddens[index].reshape(half_rows, piece),
                wdn_v[p * piece : (p + 1) * piece, :],
                preferred_element_type=F32,
            )
        send_tp("down", h, product * scale_squared, down_part, down_got, d_send, d_recv)

    def finish(h):
        total = sum_tp("down", h, down_part, down_got)
        ended = (mixed[h].astype(F32) + total).astype(BF16)
        for z in range(n_kv):
            result[z * own + h * share : z * own + (h + 1) * share, :] = ended[
                z * share : (z + 1) * share
            ]

    def settle_projections():
        wait_send(stream_copies)
        wait_send(extra_copies)
        scatter_p.finish(halves * chunks)
        gather_g.finish(halves * chunks)

    def settle_hidden():
        for name in ("mix", "block", "square"):
            for h in range(halves):
                wait_send(copies_of[name, h])
        scatter_u.finish(halves * pieces)
        gather_h.finish(halves * pieces)

    last = chunks - 1
    project_relay(0, 0)
    for c in range(chunks):
        if c < last:
            project_relay(0, c + 1)
        heads(0, c)
        if halves > 1:
            project_start(1, c)
    if halves == 1:
        for c in range(chunks):
            gated_forward(0, c)
        out_project(0)
        mix(0)
        settle_projections()
        up(0)
        for p in range(pieces):
            up_relay(0, p)
            activate(0, p)
        for p in range(pieces):
            hidden_forward(0, p)
        down(0)
    else:
        project_relay(1, 0)
        gated_forward(0, 0)
        for c in range(chunks):
            if c < last:
                project_relay(1, c + 1)
            heads(1, c)
            if c + 1 < last:
                gated_forward(0, c + 1)
            if c == last - 1:
                gated_forward(0, last)
                out_project(0)
        gated_forward(1, 0)
        mix(0)
        for c in range(1, chunks):
            gated_forward(1, c)
        out_project(1)
        settle_projections()
        up(0)
        mix(1)
        up_relay(0, 0)
        up(1)
        for p in range(1, pieces):
            up_relay(0, p)
        for p in range(pieces):
            activate(0, p)
        for p in range(pieces):
            up_relay(1, p)
        for p in range(pieces):
            hidden_forward(0, p)
        for p in range(pieces):
            activate(1, p)
        down(0)
        for p in range(pieces):
            hidden_forward(1, p)
        finish(0)
        down(1)
    settle_hidden()
    finish(halves - 1)
    for h in range(halves):
        wait_send(copies_of["down", h])


def store_kernel(result_v, state_v, result, state, sems):
    parts = sems.shape[0] - 1
    each = state_v.shape[0] // parts
    copies = [
        pltpu.make_async_copy(
            state_v.at[i * each : (i + 1) * each], state.at[i * each : (i + 1) * each], sems.at[i]
        )
        for i in range(parts)
    ]
    copies.append(pltpu.make_async_copy(result_v, result, sems.at[parts]))
    start(copies)
    for copy in copies:
        copy.wait()


def on_device(
    n_kv, n_tp,
    stream, lengths, delta_state, q_hist, k_hist, v_hist, norm_gain,
    w_query, w_key, w_value, w_gate, w_beta, w_decay,
    conv_query, conv_key, conv_value, decay_log, time_bias, out_gain,
    w_out, mlp_gain, w_up, w_down,
):
    width = norm_gain.shape[0]
    rows, own_cols = stream.shape
    own, heads_own, head = delta_state.shape[:3]
    key_cols = q_hist.shape[2]
    value_cols = v_hist.shape[2]
    block = w_query.shape[0]
    heads_all = w_beta.shape[1]
    taps = conv_query.shape[0]
    chunks = key_cols // head
    repeat = heads_own // chunks
    span = repeat * head
    field = 2 * head + 2 * span
    units = w_up.shape[1]
    seqs = min(8, own)
    halves = 2 if own % (4 * seqs) == 0 else 1
    share = own // halves
    half_rows = n_kv * share
    pieces = 4 // halves
    piece = units // pieces
    ids = halves * chunks
    shares = halves * pieces
    vmem = pl.BlockSpec(memory_space=pltpu.VMEM)
    hbm = pl.BlockSpec(memory_space=pltpu.HBM)
    dma = pltpu.SemaphoreType.DMA
    gain_shape = (width // LANES, LANES)
    ins = (
        stream, lengths[None], norm_gain.reshape(gain_shape), decay_log[None], time_bias[None],
        out_gain[None], mlp_gain.reshape(gain_shape),
        w_beta.T, w_decay.T, w_query, w_key, w_value, w_gate,
        *(jnp.transpose(hist, (1, 0, 2)) for hist in (q_hist, k_hist, v_hist)),
        conv_query, conv_key, conv_value, w_out, w_up, w_down, delta_state,
    )

    def buffer(*dims, dtype=BF16):
        return pltpu.VMEM(dims, dtype)

    result, new_state = pl.pallas_call(
        functools.partial(layer_kernel, n_kv, n_tp, width, head, repeat, chunks, pieces, halves),
        out_shape=(
            pltpu.VMEM((rows, own_cols), BF16),
            pltpu.VMEM(delta_state.shape, F32),
        ),
        in_specs=[hbm] * len(ins),
        out_specs=(vmem, vmem),
        scratch_shapes=[
            buffer(rows, own_cols), buffer(1, own, dtype=jnp.int32), buffer(*gain_shape),
            buffer(1, heads_all, dtype=F32), buffer(1, heads_all, dtype=F32),
            buffer(1, head), buffer(*gain_shape),
            buffer(heads_all, block), buffer(heads_all, block),
            buffer(block, key_cols), buffer(block, key_cols),
            buffer(block, value_cols), buffer(block, value_cols),
            buffer(taps - 1, own, key_cols), buffer(taps - 1, own, key_cols),
            buffer(taps - 1, own, value_cols),
            buffer(taps, key_cols), buffer(taps, key_cols), buffer(taps, value_cols),
            buffer(*w_out.shape), buffer(*w_up.shape), buffer(*w_down.shape),
            buffer(*gain_shape, dtype=F32), buffer(8, LANES, dtype=F32),
            buffer(n_tp, rows, own_cols),
            buffer(n_kv, own, LANES, dtype=F32), buffer(n_kv - 1, own, LANES, dtype=F32),
            buffer(ids, n_kv, share, field), buffer(ids, n_kv - 1, share, field),
            buffer(ids, share, field), buffer(ids, share, field),
            buffer(share // seqs, seqs, span, dtype=F32),
            buffer(ids, share, span), buffer(ids, n_kv, share, span),
            buffer(halves, n_tp, half_rows, own_cols), buffer(halves, n_tp - 1, half_rows, own_cols),
            buffer(halves, half_rows, own_cols), buffer(halves, n_tp, half_rows, own_cols),
            buffer(halves, 8, rows, dtype=F32), buffer(halves, n_kv, 8, rows, dtype=F32),
            buffer(shares, n_kv, share, piece), buffer(shares, n_kv - 1, share, piece),
            buffer(shares, share, piece), buffer(shares, share, piece),
            buffer(shares, share, piece), buffer(shares, n_kv, share, piece),
            buffer(halves, n_tp, half_rows, own_cols), buffer(halves, n_tp - 1, half_rows, own_cols),
            dma((22,)), dma((chunks,)),
            dma((n_tp - 1,)), dma((n_tp - 1,)),
            dma((n_kv - 1,)), dma((n_kv - 1,)),
            dma((ids, n_kv - 1)), dma((ids, n_kv - 1)), dma((ids,)),
            dma((ids, n_kv - 1)), dma((ids, n_kv - 1)), dma((ids, n_kv)),
            dma((halves, n_tp - 1)), dma((halves, n_tp - 1)),
            dma((halves, n_tp - 1)), dma((halves, n_tp - 1)),
            dma((halves, n_kv - 1)), dma((halves, n_kv - 1)),
            dma((shares, n_kv - 1)), dma((shares, n_kv - 1)), dma((shares,)),
            dma((shares, n_kv - 1)), dma((shares, n_kv - 1)), dma((shares, n_kv)),
            dma((halves, n_tp - 1)), dma((halves, n_tp - 1)),
        ],
        compiler_params=pltpu.CompilerParams(
            collective_id=0, has_side_effects=True,
            vmem_limit_bytes=67043328 - delta_state.size * 4 - 2**18,
        ),
        name="layer",
    )(*ins)
    return pl.pallas_call(
        store_kernel,
        out_shape=(
            jax.ShapeDtypeStruct(result.shape, BF16),
            jax.ShapeDtypeStruct(delta_state.shape, F32),
        ),
        in_specs=[vmem, vmem],
        out_specs=(hbm, hbm),
        scratch_shapes=[dma((min(own, 8) + 1,))],
        compiler_params=pltpu.CompilerParams(vmem_limit_bytes=2**20),
        name="store",
    )(result, new_state)


def solution(mesh):
    in_specs = (
        P("grp", ("kv", "tp")),
        P(("grp", "kv")),
        P(("grp", "kv"), "tp", None, None),
        P(("grp", "kv"), None, "tp"),
        P(("grp", "kv"), None, "tp"),
        P(("grp", "kv"), None, "tp"),
        P(),
        P("kv", "tp"),
        P("kv", "tp"),
        P("kv", "tp"),
        P("kv", "tp"),
        P(),
        P(),
        P(),
        P(),
        P(),
        P(),
        P(),
        P(),
        P("tp", "kv"),
        P(),
        P("kv", "tp"),
        P("tp", "kv"),
    )
    out_specs = (P("grp", ("kv", "tp")), P(("grp", "kv"), "tp", None, None))
    return jax.shard_map(
        functools.partial(on_device, mesh.shape["kv"], mesh.shape["tp"]),
        mesh=mesh, in_specs=in_specs, out_specs=out_specs, check_vma=False,
    )
```

```python
import functools

import jax
import jax.numpy as jnp
from jax import lax
from jax.experimental import pallas as pl
from jax.experimental.pallas import tpu as pltpu
from jax.sharding import PartitionSpec as P

EPSILON = 1e-06
MESH = pl.DeviceIdType.MESH
F32 = jnp.float32
BF16 = jnp.bfloat16
LANES = 128
LEAD = 2
DIRECT_LAST = 1
CONTRACT_LAST = (((1,), (1,)), ((), ()))


def greet(axes):
    barrier = pltpu.get_barrier_semaphore()
    total = 0
    for name, size in axes:
        me = lax.axis_index(name)
        for step in range(1, size):
            pl.semaphore_signal(
                barrier, inc=1, device_id={name: lax.rem(me + step, size)}, device_id_type=MESH
            )
            total += 1
    pl.semaphore_wait(barrier, total)


def order(size):
    return sorted(range(1, size), key=lambda step: -min(step, size - step))


def remote(name, peer, src, dst, send, recv):
    return pltpu.make_async_remote_copy(
        src_ref=src, dst_ref=dst, send_sem=send, recv_sem=recv,
        device_id={name: peer}, device_id_type=MESH,
    )


def scatter_copies(name, size, src, dst, send, recv):
    me = lax.axis_index(name)
    copies = []
    for step in order(size):
        peer = lax.rem(me + step, size)
        copies.append(
            remote(name, peer, src.at[peer], dst.at[step - 1], send.at[step - 1], recv.at[step - 1])
        )
    return copies


def gather_copies(name, size, src, dst, send, recv):
    me = lax.axis_index(name)
    copies = []
    for step in order(size):
        peer = lax.rem(me + step, size)
        copies.append(
            remote(name, peer, src, dst.at[me], send.at[step - 1], recv.at[step - 1])
        )
    return copies


def start(copies):
    for copy in copies:
        copy.start()


def wait_recv(copies):
    for copy in copies:
        copy.wait_recv()


def wait_send(copies):
    for copy in copies:
        copy.wait_send()


def unless(conditions, action):
    if not conditions:
        action()
        return
    skip = functools.reduce(jnp.logical_or, conditions)
    pl.when(jnp.logical_not(skip))(action)


class LineScatter:
    def __init__(
        self, name, size, group, part, got, relay_in, relay_out, send, recv, relay_recv
    ):
        self.name, self.size, self.me = name, size, lax.axis_index(name)
        self.part, self.got = part, got
        self.relay_in, self.relay_out = relay_in, relay_out
        self.send, self.recv, self.relay_recv = send, recv, relay_recv
        self.chunks, self.group = part.shape[0], group
        self.relays = size >= 4

    def copy(self, c, step, src=None):
        peer = lax.rem(self.me + step, self.size)
        src = self.part.at[c, peer] if src is None else src
        return remote(
            self.name, peer, src, self.got.at[c, step - 1],
            self.send.at[c, step - 1], self.recv.at[c, step - 1],
        )

    def ends(self):
        last = self.size - 1
        return ((0, last, last, 1, last - 1), (last, 0, 1, last - 1, 2))

    def clear(self):
        if not self.relays:
            return
        for end, _, step, _, _ in self.ends():
            slot = self.size - step - 1

            @pl.when(self.me == end)
            def _():
                self.got[:, slot] = jnp.zeros(self.got.shape[:1] + self.got.shape[2:], self.got.dtype)

    def relay_copy(self, c, block, step, neighbour):
        return remote(
            self.name, neighbour, self.part.at[c, block], self.relay_in.at[c],
            self.send.at[c, step - 1], self.relay_recv.at[c],
        )

    def start(self, c):
        if self.relays:
            for end, block, step, neighbour, _ in self.ends():
                pl.when(self.me == end)(self.relay_copy(c, block, step, neighbour).start)
        for step in order(self.size):
            skips = []
            if self.relays:
                for end, _, far, neighbour, last in self.ends():
                    if step == far:
                        skips.append(self.me == end)
                    if step == last or c % self.group >= LEAD:
                        skips.append(self.me == neighbour)
            unless(skips, self.copy(c, step).start)

    def relay(self, c):
        if not self.relays:
            return
        for end, block, step, neighbour, last in self.ends():

            @pl.when(self.me == neighbour)
            def _():
                self.relay_copy(c, block, step, neighbour).wait_recv()
                total = self.relay_in[c].astype(F32) + self.part[c, block].astype(F32)
                self.relay_out[c] = total.astype(self.relay_out.dtype)
                self.copy(c, last, self.relay_out.at[c]).start()
                if c + LEAD < self.chunks and (c + LEAD) % self.group >= LEAD:
                    for hop in order(self.size):
                        if hop != last:
                            self.copy(c + LEAD, hop).start()

    def total(self, c):
        for step in order(self.size):
            skips = []
            if self.relays:
                for end, _, far, _, _ in self.ends():
                    if step == self.size - far:
                        skips.append(self.me == end)
            unless(skips, self.copy(c, step).wait_recv)
        total = self.part[c, self.me].astype(F32)
        for slot in range(self.size - 1):
            total = total + self.got[c, slot].astype(F32)
        return total

    def finish(self, chunks):
        for c in range(chunks):
            for step in range(1, self.size):
                self.copy(c, step).wait_send()


class LineGather:
    def __init__(self, name, size, group, mine, everyone, send, recv, relay_send):
        self.name, self.size, self.me = name, size, lax.axis_index(name)
        self.mine, self.everyone = mine, everyone
        self.send, self.recv, self.relay_send = send, recv, relay_send
        self.relays = size >= 3
        self.direct = [c for c in range(mine.shape[0]) if c % group >= group - DIRECT_LAST]

    def copy(self, c, step):
        peer = lax.rem(self.me + step, self.size)
        return remote(
            self.name, peer, self.mine.at[c], self.everyone.at[c, self.me],
            self.send.at[c, step - 1], self.recv.at[c, step - 1],
        )

    def skips(self, c, step):
        if not self.relays or c in self.direct:
            return []
        skips = []
        if step != self.size - 1:
            skips.append(self.me == self.size - step)
        if step != 1:
            skips.append(self.me == self.size - 1 - step)
        return skips

    def start(self, c):
        for step in order(self.size):
            unless(self.skips(c, step), self.copy(c, step).start)

    def forwards(self):
        last = self.size - 1
        return ((1, 0, range(2, self.size)), (last - 1, last, range(last - 2, -1, -1)))

    def onward(self, c, end, source):
        step = (end - source) % self.size
        block = self.everyone.at[c, source]
        return remote(
            self.name, end, block, block, self.relay_send.at[c, source], self.recv.at[c, step - 1]
        )

    def forward(self, c):
        if not self.relays or c in self.direct:
            return
        for neighbour, end, sources in self.forwards():

            @pl.when(self.me == neighbour)
            def _():
                for source in sources:
                    step = (neighbour - source) % self.size
                    self.copy(c, step).wait_recv()
                    self.onward(c, end, source).start()

    def wait(self, c):
        for step in order(self.size):
            skips = []
            if self.relays and c not in self.direct:
                if step != 1:
                    skips.append(self.me == 1)
                if step != self.size - 1:
                    skips.append(self.me == self.size - 2)
            unless(skips, self.copy(c, step).wait_recv)

    def finish(self, chunks):
        for c in range(chunks):
            for step in range(1, self.size):
                unless(self.skips(c, step), self.copy(c, step).wait_send)
            if self.relays and c not in self.direct:
                for neighbour, end, sources in self.forwards():

                    @pl.when(self.me == neighbour)
                    def _():
                        for source in sources:
                            self.onward(c, end, source).wait_send()


def silu(values):
    return values * jax.nn.sigmoid(values)


def softplus(values):
    return jnp.maximum(values, 0.0) + jnp.log1p(jnp.exp(-jnp.abs(values)))


def row_blocks(name, columns):
    return pl.ds(pl.multiple_of(lax.axis_index(name) * columns, LANES), columns)


def layer_kernel(
    n_kv, n_tp, width, head, repeat, chunks, pieces, halves,
    stream, lengths, gain, decay_log, time_bias, out_gain, mlp_gain,
    w_b, w_d, w_q, w_k, w_v, w_g, q_hist, k_hist, v_hist, conv_q, conv_k, conv_v,
    w_out, w_up, w_down, state,
    result, new_state,
    stream_v, len_v, gain_v, dlog_v, bias_v, ogain_v, mgain_v,
    wb_v, wd_v, wq_v, wk_v, wv_v, wg_v, hist_q, hist_k, hist_v, convq_v, convk_v, convv_v,
    wo_v, wu_v, wdn_v,
    gains, params, streams, part_e, got_e,
    part_p, got_p, relay_pi, relay_po,
    readouts,
    mine, gathered, mix_part, mix_got, mixed, blocks, sq_part, sq_got,
    up_part, up_got, relay_ui, relay_uo, hidden, hiddens, down_part, down_got,
    load_sem, state_sem, s_send, s_recv, e_send, e_recv,
    p_send, p_recv, p_relay, g_send, g_recv, g_relay,
    m_send, m_recv, b_send, b_recv, q_send, q_recv,
    u_send, u_recv, u_relay, h_send, h_recv, h_relay, d_send, d_recv,
):
    kv = lax.axis_index("kv")
    tp = lax.axis_index("tp")
    rows, own_cols = stream_v.shape
    own = rows // n_kv
    share = own // halves
    half_rows = n_kv * share
    block = wq_v.shape[0]
    heads_all = w_b.shape[0]
    heads_own = chunks * repeat
    span = repeat * head
    block_cols = row_blocks("kv", block)

    sources = (
        (stream, stream_v),
        (gain, gain_v),
        (w_b.at[:, block_cols], wb_v), (w_d.at[:, block_cols], wd_v),
        (w_q, wq_v), (w_k, wk_v), (w_v, wv_v), (w_g, wg_v),
        (lengths, len_v), (decay_log, dlog_v), (time_bias, bias_v),
        (out_gain, ogain_v), (mlp_gain, mgain_v),
        (q_hist, hist_q), (k_hist, hist_k), (v_hist, hist_v),
        (conv_q.at[:, row_blocks("tp", convq_v.shape[1])], convq_v),
        (conv_k.at[:, row_blocks("tp", convk_v.shape[1])], convk_v),
        (conv_v.at[:, row_blocks("tp", convv_v.shape[1])], convv_v),
        (w_out, wo_v), (w_up, wu_v), (w_down, wdn_v),
    )
    loads = [pltpu.make_async_copy(src, dst, load_sem.at[i]) for i, (src, dst) in enumerate(sources)]
    state_loads = [
        pltpu.make_async_copy(
            state.at[:, c * repeat : (c + 1) * repeat],
            new_state.at[:, c * repeat : (c + 1) * repeat],
            state_sem.at[c],
        )
        for c in range(chunks)
    ]
    start(loads[:19])
    start(state_loads)
    start(loads[19:])

    scatter_p = LineScatter("kv", n_kv, halves * chunks, part_p, got_p, relay_pi, relay_po, p_send, p_recv, p_relay)
    gather_g = LineGather("kv", n_kv, chunks, mine, gathered, g_send, g_recv, g_relay)
    scatter_u = LineScatter("kv", n_kv, pieces, up_part, up_got, relay_ui, relay_uo, u_send, u_recv, u_relay)
    gather_h = LineGather("kv", n_kv, pieces, hidden, hiddens, h_send, h_recv, h_relay)
    scatter_p.clear()
    scatter_u.clear()

    greet((("kv", n_kv), ("tp", n_tp)))
    loads[0].wait()
    stream_copies = gather_copies("tp", n_tp, stream_v, streams, s_send, s_recv)
    start(stream_copies)
    streams[tp] = stream_v[...]
    loads[1].wait()

    def gain_row(values):
        gains[...] = values[...].astype(F32)
        lines = block // LANES
        return jnp.concatenate(
            [gains[pl.ds(kv * lines + j, 1), :] for j in range(lines)], axis=1
        )

    norm_row = gain_row(gain_v)
    wait_recv(stream_copies)

    wide = jnp.concatenate([streams[t] for t in range(n_tp)], axis=1).astype(F32)
    scaled = (wide * norm_row).astype(BF16)

    def extras():
        loads[2].wait()
        loads[3].wait()
        beta = lax.dot_general(scaled, wb_v[...], CONTRACT_LAST, preferred_element_type=F32)
        decay = lax.dot_general(scaled, wd_v[...], CONTRACT_LAST, preferred_element_type=F32)
        squares = jnp.sum(wide * wide, axis=1, keepdims=True)
        coarse = squares.astype(BF16)
        fine = (squares - coarse.astype(F32)).astype(BF16)
        spare = (LANES - 2 * heads_all) // 2
        part_e[...] = jnp.concatenate(
            [
                beta.astype(BF16), decay.astype(BF16),
                jnp.broadcast_to(coarse, (rows, spare)), jnp.broadcast_to(fine, (rows, spare)),
            ],
            axis=1,
        ).reshape(n_kv, own, LANES)
        copies = scatter_copies("kv", n_kv, part_e, got_e, e_send, e_recv)
        start(copies)
        return copies

    for copy in loads[4:8]:
        copy.wait()
    fields = ((wq_v, head, 0), (wk_v, head, head), (wv_v, span, 2 * head), (wg_v, span, 2 * head + span))
    for c in range(chunks):
        for weight, size, offset in fields:
            product = jnp.dot(
                scaled, weight[:, c * size : (c + 1) * size], preferred_element_type=F32
            )
            split = product.reshape(n_kv, own, size).astype(BF16)
            for h in range(halves):
                part_p[h * chunks + c, :, :, offset : offset + size] = split[
                    :, h * share : (h + 1) * share
                ]
        scatter_p.start(c)
        if c == 0:
            extra_copies = extras()

    for copy in loads[8:19]:
        copy.wait()
    lens_row = jnp.broadcast_to(len_v[...].astype(F32), (own, own))
    diagonal = lax.broadcasted_iota(jnp.int32, (own, own), 0) == lax.broadcasted_iota(
        jnp.int32, (own, own), 1
    )
    length = jnp.sum(jnp.where(diagonal, lens_row, 0.0), axis=1, keepdims=True)

    def history(hist, taps):
        total = None
        count = taps.shape[0]
        for r in range(count - 1):
            live = length >= float(count - r)
            term = jnp.where(live, hist[r].astype(F32) * taps[r : r + 1, :], 0.0)
            total = term if total is None else total + term
        return total

    taps_q = convq_v[...].astype(F32)
    taps_k = convk_v[...].astype(F32)
    taps_v = convv_v[...].astype(F32)
    past_q = history(hist_q, taps_q)
    past_k = history(hist_k, taps_k)
    past_v = history(hist_v, taps_v)
    final = taps_q.shape[0] - 1

    params[...] = jnp.zeros(params.shape, F32)
    params[0:1, :heads_all] = dlog_v[...]
    params[1:2, :heads_all] = bias_v[...]
    shift = tp * heads_own
    own_params = pltpu.roll(params[...], lax.rem(LANES - shift, LANES), 1)

    scatter_p.relay(0)
    wait_recv(extra_copies)
    extra = part_e[kv].astype(F32)
    for slot in range(n_kv - 1):
        extra = extra + got_e[slot].astype(F32)
    fine_at = heads_all + LANES // 2
    square_sum = extra[:, 2 * heads_all : 2 * heads_all + 1] + extra[:, fine_at : fine_at + 1]
    row_scale = lax.rsqrt(square_sum / width + EPSILON)
    terms = extra * row_scale
    own_beta = pltpu.roll(terms, lax.rem(LANES - shift, LANES), 1)
    own_decay = pltpu.roll(terms, lax.rem(2 * LANES - heads_all - shift, LANES), 1)
    fade = jnp.exp(-jnp.exp(own_params[0:1, :]) * softplus(own_decay + own_params[1:2, :]))
    fade = jnp.where(length == 1.0, 0.0, fade)
    strength = jax.nn.sigmoid(own_beta)
    gain_out = ogain_v[...].astype(F32)

    def unit(values, factor):
        return values * (
            lax.rsqrt(jnp.sum(values * values, axis=1, keepdims=True) + EPSILON) * factor
        )

    seqs = readouts.shape[1]

    def heads(h, c):
        index = h * chunks + c
        these = slice(h * share, (h + 1) * share)
        total = scatter_p.total(index) * row_scale[these]
        narrow = slice(c * head, (c + 1) * head)
        broad = slice(c * span, (c + 1) * span)
        query = unit(
            silu(total[:, :head] * taps_q[final : final + 1, narrow] + past_q[these, narrow]),
            head ** (-0.5),
        )
        key = unit(
            silu(total[:, head : 2 * head] * taps_k[final : final + 1, narrow] + past_k[these, narrow]),
            1.0,
        )
        values = silu(
            total[:, 2 * head : 2 * head + span] * taps_v[final : final + 1, broad] + past_v[these, broad]
        )
        gate = silu(total[:, 2 * head + span :])
        dot = jnp.sum(query * key, axis=1, keepdims=True)
        owned = range(c * repeat, (c + 1) * repeat)

        def widen(columns):
            return jnp.concatenate(
                [jnp.broadcast_to(column, (share, head)) for column in columns], axis=1
            )

        dots = widen([dot] * repeat)
        fades = widen([fade[these, v : v + 1] for v in owned])
        strengths = widen([strength[these, v : v + 1] for v in owned])
        keys_t = key.T
        line = lax.broadcasted_iota(jnp.int32, (seqs, span), 0)
        if h == 0:
            state_loads[c].wait()

        def ask(g):
            some = slice(g * seqs, (g + 1) * seqs)
            both = jnp.concatenate([key[some], query[some]], axis=0).astype(BF16)
            recalled = jnp.zeros((seqs, span), F32)
            asked = jnp.zeros((seqs, span), F32)
            for s in range(seqs):
                q = h * share + g * seqs + s
                held = jnp.concatenate([new_state[q, v] for v in owned], axis=1)
                answer = jnp.dot(both, held.astype(BF16), preferred_element_type=F32)
                recalled = jnp.where(line == s, answer[:seqs], recalled)
                asked = jnp.where(line == s, answer[seqs:], asked)
            faded = fades[some]
            update = strengths[some] * (values[some] - faded * recalled)
            readouts[g] = faded * asked + dots[some] * update
            return faded, update

        def apply(g, faded, update):
            for s in range(seqs):
                q = h * share + g * seqs + s
                near = g * seqs + s
                wide_key = jnp.broadcast_to(keys_t[:, near : near + 1], (head, head))
                for j, v in enumerate(owned):
                    cols = slice(j * head, (j + 1) * head)
                    new_state[q, v] = (
                        new_state[q, v] * faded[s : s + 1, cols] + wide_key * update[s : s + 1, cols]
                    )

        groups = share // seqs
        ready = ask(0)
        for g in range(groups):
            later = ask(g + 1) if g + 1 < groups else None
            apply(g, *ready)
            ready = later

        for j in range(repeat):
            cols = slice(j * head, (j + 1) * head)
            one = readouts[:, :, cols].reshape(share, head)
            normed = one * lax.rsqrt(jnp.mean(one * one, axis=1, keepdims=True) + EPSILON)
            mine[index, :, cols] = (normed * gain_out * gate[:, cols]).astype(BF16)
        gather_g.start(index)
        gathered[index, kv] = mine[index]

    def project_relay(h, c):
        scatter_p.relay(h * chunks + c)

    def project_start(h, c):
        scatter_p.start(h * chunks + c)

    def gated_forward(h, c):
        gather_g.forward(h * chunks + c)

    copies_of = {}

    def send_tp(name, h, product, part, got, send_sem, recv_sem):
        for t in range(n_tp):
            part[h, t] = product[:, t * own_cols : (t + 1) * own_cols].astype(BF16)
        copies = scatter_copies("tp", n_tp, part.at[h], got.at[h], send_sem.at[h], recv_sem.at[h])
        start(copies)
        copies_of[name, h] = copies

    def sum_tp(name, h, part, got):
        wait_recv(copies_of[name, h])
        total = part[h, tp].astype(F32)
        for slot in range(n_tp - 1):
            total = total + got[h, slot].astype(F32)
        return total

    def out_project(h):
        if h == 0:
            loads[19].wait()
        product = jnp.zeros((half_rows, wo_v.shape[1]), F32)
        for c in range(chunks):
            gather_g.wait(h * chunks + c)
            product = product + jnp.dot(
                gathered[h * chunks + c].reshape(half_rows, span),
                wo_v[c * span : (c + 1) * span, :],
                preferred_element_type=F32,
            )
        send_tp("mix", h, product, mix_part, mix_got, m_send, m_recv)

    def mix(h):
        total = sum_tp("mix", h, mix_part, mix_got)
        before = jnp.concatenate(
            [stream_v[z * own + h * share : z * own + (h + 1) * share, :] for z in range(n_kv)], axis=0
        )
        mixed_own = (before.astype(F32) + total).astype(BF16)
        mixed[h] = mixed_own
        copies = gather_copies("tp", n_tp, mixed.at[h], blocks.at[h], b_send.at[h], b_recv.at[h])
        start(copies)
        copies_of["block", h] = copies
        blocks[h, tp] = mixed_own

    mlp_row = gain_row(mgain_v)
    piece = wu_v.shape[1] // pieces
    corner = lax.broadcasted_iota(jnp.int32, (half_rows, half_rows), 0) == lax.broadcasted_iota(
        jnp.int32, (half_rows, half_rows), 1
    )

    def up(h):
        if h == 0:
            loads[20].wait()
        wait_recv(copies_of["block", h])
        wide = jnp.concatenate([blocks[h, t] for t in range(n_tp)], axis=1).astype(F32)
        scaled = (wide * mlp_row).astype(BF16)
        for p in range(pieces):
            product = jnp.dot(
                scaled, wu_v[:, p * piece : (p + 1) * piece], preferred_element_type=F32
            )
            up_part[h * pieces + p] = product.reshape(n_kv, share, piece).astype(BF16)
            scatter_u.start(h * pieces + p)
        squares = jnp.sum(wide * wide, axis=1, keepdims=True)
        flat = jnp.sum(jnp.where(corner, squares, 0.0), axis=0, keepdims=True)
        sq_part[h, :, :half_rows] = jnp.broadcast_to(flat, (sq_part.shape[1], half_rows))
        copies = gather_copies("kv", n_kv, sq_part.at[h], sq_got.at[h], q_send.at[h], q_recv.at[h])
        start(copies)
        copies_of["square", h] = copies
        sq_got[h, kv, :, :half_rows] = sq_part[h, :, :half_rows]

    def up_relay(h, p):
        scatter_u.relay(h * pieces + p)

    def activate(h, p):
        index = h * pieces + p
        active = jnp.maximum(scatter_u.total(index), 0.0)
        active = (active * active).astype(BF16)
        hidden[index] = active
        gather_h.start(index)
        hiddens[index, kv] = active

    def hidden_forward(h, p):
        gather_h.forward(h * pieces + p)

    def down(h):
        if h == 0:
            loads[21].wait()
        wait_recv(copies_of["square", h])
        square_sum = sq_got[h, 0, :, :half_rows]
        for z in range(1, n_kv):
            square_sum = square_sum + sq_got[h, z, :, :half_rows]
        spread = jnp.broadcast_to(
            1.0 / (square_sum[0:1, :] / width + EPSILON), (half_rows, half_rows)
        )
        scale_squared = jnp.sum(jnp.where(corner, spread, 0.0), axis=1, keepdims=True)
        product = jnp.zeros((half_rows, wdn_v.shape[1]), F32)
        for p in range(pieces):
            index = h * pieces + p
            gather_h.wait(index)
            product = product + jnp.dot(
                hiddens[index].reshape(half_rows, piece),
                wdn_v[p * piece : (p + 1) * piece, :],
                preferred_element_type=F32,
            )
        send_tp("down", h, product * scale_squared, down_part, down_got, d_send, d_recv)

    def finish(h):
        total = sum_tp("down", h, down_part, down_got)
        ended = (mixed[h].astype(F32) + total).astype(BF16)
        for z in range(n_kv):
            result[z * own + h * share : z * own + (h + 1) * share, :] = ended[
                z * share : (z + 1) * share
            ]

    def settle_projections():
        wait_send(stream_copies)
        wait_send(extra_copies)
        scatter_p.finish(halves * chunks)
        gather_g.finish(halves * chunks)

    def settle_hidden():
        for name in ("mix", "block", "square"):
            for h in range(halves):
                wait_send(copies_of[name, h])
        scatter_u.finish(halves * pieces)
        gather_h.finish(halves * pieces)

    last = chunks - 1
    for c in range(chunks):
        if c < last:
            project_relay(0, c + 1)
        heads(0, c)
        if halves > 1:
            project_start(1, c)
    if halves == 1:
        for c in range(chunks):
            gated_forward(0, c)
        out_project(0)
        mix(0)
        settle_projections()
        up(0)
        for p in range(pieces):
            up_relay(0, p)
            activate(0, p)
        for p in range(pieces):
            hidden_forward(0, p)
        down(0)
    else:
        project_relay(1, 0)
        gated_forward(0, 0)
        for c in range(chunks):
            if c < last:
                project_relay(1, c + 1)
            heads(1, c)
            if c + 1 < last:
                gated_forward(0, c + 1)
            if c == last - 1:
                gated_forward(0, last)
                out_project(0)
        gated_forward(1, 0)
        mix(0)
        for c in range(1, chunks):
            gated_forward(1, c)
        out_project(1)
        settle_projections()
        up(0)
        mix(1)
        up_relay(0, 0)
        up(1)
        for p in range(1, pieces):
            up_relay(0, p)
        for p in range(pieces):
            activate(0, p)
            up_relay(1, p)
        for p in range(pieces):
            hidden_forward(0, p)
        for p in range(pieces):
            activate(1, p)
        down(0)
        for p in range(pieces):
            hidden_forward(1, p)
        finish(0)
        down(1)
    settle_hidden()
    finish(halves - 1)
    for h in range(halves):
        wait_send(copies_of["down", h])


def store_kernel(result_v, state_v, result, state, sems):
    parts = sems.shape[0] - 1
    each = state_v.shape[0] // parts
    copies = [
        pltpu.make_async_copy(
            state_v.at[i * each : (i + 1) * each], state.at[i * each : (i + 1) * each], sems.at[i]
        )
        for i in range(parts)
    ]
    copies.append(pltpu.make_async_copy(result_v, result, sems.at[parts]))
    start(copies)
    for copy in copies:
        copy.wait()


def on_device(
    n_kv, n_tp,
    stream, lengths, delta_state, q_hist, k_hist, v_hist, norm_gain,
    w_query, w_key, w_value, w_gate, w_beta, w_decay,
    conv_query, conv_key, conv_value, decay_log, time_bias, out_gain,
    w_out, mlp_gain, w_up, w_down,
):
    width = norm_gain.shape[0]
    rows, own_cols = stream.shape
    own, heads_own, head = delta_state.shape[:3]
    key_cols = q_hist.shape[2]
    value_cols = v_hist.shape[2]
    block = w_query.shape[0]
    heads_all = w_beta.shape[1]
    taps = conv_query.shape[0]
    chunks = key_cols // head
    repeat = heads_own // chunks
    span = repeat * head
    field = 2 * head + 2 * span
    units = w_up.shape[1]
    seqs = min(8, own)
    halves = 2 if own % (4 * seqs) == 0 else 1
    share = own // halves
    half_rows = n_kv * share
    pieces = 4 // halves
    piece = units // pieces
    ids = halves * chunks
    shares = halves * pieces
    vmem = pl.BlockSpec(memory_space=pltpu.VMEM)
    hbm = pl.BlockSpec(memory_space=pltpu.HBM)
    dma = pltpu.SemaphoreType.DMA
    gain_shape = (width // LANES, LANES)
    ins = (
        stream, lengths[None], norm_gain.reshape(gain_shape), decay_log[None], time_bias[None],
        out_gain[None], mlp_gain.reshape(gain_shape),
        w_beta.T, w_decay.T, w_query, w_key, w_value, w_gate,
        *(jnp.transpose(hist, (1, 0, 2)) for hist in (q_hist, k_hist, v_hist)),
        conv_query, conv_key, conv_value, w_out, w_up, w_down, delta_state,
    )

    def buffer(*dims, dtype=BF16):
        return pltpu.VMEM(dims, dtype)

    result, new_state = pl.pallas_call(
        functools.partial(layer_kernel, n_kv, n_tp, width, head, repeat, chunks, pieces, halves),
        out_shape=(
            pltpu.VMEM((rows, own_cols), BF16),
            pltpu.VMEM(delta_state.shape, F32),
        ),
        in_specs=[hbm] * len(ins),
        out_specs=(vmem, vmem),
        scratch_shapes=[
            buffer(rows, own_cols), buffer(1, own, dtype=jnp.int32), buffer(*gain_shape),
            buffer(1, heads_all, dtype=F32), buffer(1, heads_all, dtype=F32),
            buffer(1, head), buffer(*gain_shape),
            buffer(heads_all, block), buffer(heads_all, block),
            buffer(block, key_cols), buffer(block, key_cols),
            buffer(block, value_cols), buffer(block, value_cols),
            buffer(taps - 1, own, key_cols), buffer(taps - 1, own, key_cols),
            buffer(taps - 1, own, value_cols),
            buffer(taps, key_cols), buffer(taps, key_cols), buffer(taps, value_cols),
            buffer(*w_out.shape), buffer(*w_up.shape), buffer(*w_down.shape),
            buffer(*gain_shape, dtype=F32), buffer(8, LANES, dtype=F32),
            buffer(n_tp, rows, own_cols),
            buffer(n_kv, own, LANES), buffer(n_kv - 1, own, LANES),
            buffer(ids, n_kv, share, field), buffer(ids, n_kv - 1, share, field),
            buffer(ids, share, field), buffer(ids, share, field),
            buffer(share // seqs, seqs, span, dtype=F32),
            buffer(ids, share, span), buffer(ids, n_kv, share, span),
            buffer(halves, n_tp, half_rows, own_cols), buffer(halves, n_tp - 1, half_rows, own_cols),
            buffer(halves, half_rows, own_cols), buffer(halves, n_tp, half_rows, own_cols),
            buffer(halves, 8, rows, dtype=F32), buffer(halves, n_kv, 8, rows, dtype=F32),
            buffer(shares, n_kv, share, piece), buffer(shares, n_kv - 1, share, piece),
            buffer(shares, share, piece), buffer(shares, share, piece),
            buffer(shares, share, piece), buffer(shares, n_kv, share, piece),
            buffer(halves, n_tp, half_rows, own_cols), buffer(halves, n_tp - 1, half_rows, own_cols),
            dma((22,)), dma((chunks,)),
            dma((n_tp - 1,)), dma((n_tp - 1,)),
            dma((n_kv - 1,)), dma((n_kv - 1,)),
            dma((ids, n_kv - 1)), dma((ids, n_kv - 1)), dma((ids,)),
            dma((ids, n_kv - 1)), dma((ids, n_kv - 1)), dma((ids, n_kv)),
            dma((halves, n_tp - 1)), dma((halves, n_tp - 1)),
            dma((halves, n_tp - 1)), dma((halves, n_tp - 1)),
            dma((halves, n_kv - 1)), dma((halves, n_kv - 1)),
            dma((shares, n_kv - 1)), dma((shares, n_kv - 1)), dma((shares,)),
            dma((shares, n_kv - 1)), dma((shares, n_kv - 1)), dma((shares, n_kv)),
            dma((halves, n_tp - 1)), dma((halves, n_tp - 1)),
        ],
        compiler_params=pltpu.CompilerParams(
            collective_id=0, has_side_effects=True,
            vmem_limit_bytes=67043328 - delta_state.size * 4 - 2**18,
        ),
        name="layer",
    )(*ins)
    return pl.pallas_call(
        store_kernel,
        out_shape=(
            jax.ShapeDtypeStruct(result.shape, BF16),
            jax.ShapeDtypeStruct(delta_state.shape, F32),
        ),
        in_specs=[vmem, vmem],
        out_specs=(hbm, hbm),
        scratch_shapes=[dma((min(own, 8) + 1,))],
        compiler_params=pltpu.CompilerParams(vmem_limit_bytes=2**20),
        name="store",
    )(result, new_state)


def solution(mesh):
    in_specs = (
        P("grp", ("kv", "tp")),
        P(("grp", "kv")),
        P(("grp", "kv"), "tp", None, None),
        P(("grp", "kv"), None, "tp"),
        P(("grp", "kv"), None, "tp"),
        P(("grp", "kv"), None, "tp"),
        P(),
        P("kv", "tp"),
        P("kv", "tp"),
        P("kv", "tp"),
        P("kv", "tp"),
        P(),
        P(),
        P(),
        P(),
        P(),
        P(),
        P(),
        P(),
        P("tp", "kv"),
        P(),
        P("kv", "tp"),
        P("tp", "kv"),
    )
    out_specs = (P("grp", ("kv", "tp")), P(("grp", "kv"), "tp", None, None))
    return jax.shard_map(
        functools.partial(on_device, mesh.shape["kv"], mesh.shape["tp"]),
        mesh=mesh, in_specs=in_specs, out_specs=out_specs, check_vma=False,
    )
```

```python
import functools

import jax
import jax.numpy as jnp
from jax import lax
from jax.experimental import pallas as pl
from jax.experimental.pallas import tpu as pltpu
from jax.sharding import PartitionSpec as P

EPSILON = 1e-06
MESH = pl.DeviceIdType.MESH
F32 = jnp.float32
BF16 = jnp.bfloat16
LANES = 128
LEAD = 2
DIRECT_LAST = 1
CONTRACT_LAST = (((1,), (1,)), ((), ()))


def greet(axes):
    barrier = pltpu.get_barrier_semaphore()
    total = 0
    for name, size in axes:
        me = lax.axis_index(name)
        for step in range(1, size):
            pl.semaphore_signal(
                barrier, inc=1, device_id={name: lax.rem(me + step, size)}, device_id_type=MESH
            )
            total += 1
    pl.semaphore_wait(barrier, total)


def order(size):
    return sorted(range(1, size), key=lambda step: -min(step, size - step))


def remote(name, peer, src, dst, send, recv):
    return pltpu.make_async_remote_copy(
        src_ref=src, dst_ref=dst, send_sem=send, recv_sem=recv,
        device_id={name: peer}, device_id_type=MESH,
    )


def scatter_copies(name, size, src, dst, send, recv):
    me = lax.axis_index(name)
    copies = []
    for step in order(size):
        peer = lax.rem(me + step, size)
        copies.append(
            remote(name, peer, src.at[peer], dst.at[step - 1], send.at[step - 1], recv.at[step - 1])
        )
    return copies


def gather_copies(name, size, src, dst, send, recv):
    me = lax.axis_index(name)
    copies = []
    for step in order(size):
        peer = lax.rem(me + step, size)
        copies.append(
            remote(name, peer, src, dst.at[me], send.at[step - 1], recv.at[step - 1])
        )
    return copies


def start(copies):
    for copy in copies:
        copy.start()


def wait_recv(copies):
    for copy in copies:
        copy.wait_recv()


def wait_send(copies):
    for copy in copies:
        copy.wait_send()


def unless(conditions, action):
    if not conditions:
        action()
        return
    skip = functools.reduce(jnp.logical_or, conditions)
    pl.when(jnp.logical_not(skip))(action)


class LineScatter:
    def __init__(
        self, name, size, group, part, got, relay_in, relay_out, send, recv, relay_recv
    ):
        self.name, self.size, self.me = name, size, lax.axis_index(name)
        self.part, self.got = part, got
        self.relay_in, self.relay_out = relay_in, relay_out
        self.send, self.recv, self.relay_recv = send, recv, relay_recv
        self.chunks, self.group = part.shape[0], group
        self.relays = size >= 4

    def copy(self, c, step, src=None):
        peer = lax.rem(self.me + step, self.size)
        src = self.part.at[c, peer] if src is None else src
        return remote(
            self.name, peer, src, self.got.at[c, step - 1],
            self.send.at[c, step - 1], self.recv.at[c, step - 1],
        )

    def ends(self):
        last = self.size - 1
        return ((0, last, last, 1, last - 1), (last, 0, 1, last - 1, 2))

    def clear(self):
        if not self.relays:
            return
        for end, _, step, _, _ in self.ends():
            slot = self.size - step - 1

            @pl.when(self.me == end)
            def _():
                self.got[:, slot] = jnp.zeros(self.got.shape[:1] + self.got.shape[2:], self.got.dtype)

    def relay_copy(self, c, block, step, neighbour):
        return remote(
            self.name, neighbour, self.part.at[c, block], self.relay_in.at[c],
            self.send.at[c, step - 1], self.relay_recv.at[c],
        )

    def start(self, c):
        if self.relays:
            for end, block, step, neighbour, _ in self.ends():
                pl.when(self.me == end)(self.relay_copy(c, block, step, neighbour).start)
        for step in order(self.size):
            skips = []
            if self.relays:
                for end, _, far, neighbour, last in self.ends():
                    if step == far:
                        skips.append(self.me == end)
                    if step == last or c % self.group >= LEAD:
                        skips.append(self.me == neighbour)
            unless(skips, self.copy(c, step).start)

    def relay(self, c):
        if not self.relays:
            return
        for end, block, step, neighbour, last in self.ends():

            @pl.when(self.me == neighbour)
            def _():
                self.relay_copy(c, block, step, neighbour).wait_recv()
                total = self.relay_in[c].astype(F32) + self.part[c, block].astype(F32)
                self.relay_out[c] = total.astype(self.relay_out.dtype)
                self.copy(c, last, self.relay_out.at[c]).start()
                if c + LEAD < self.chunks and (c + LEAD) % self.group >= LEAD:
                    for hop in order(self.size):
                        if hop != last:
                            self.copy(c + LEAD, hop).start()

    def total(self, c):
        for step in order(self.size):
            skips = []
            if self.relays:
                for end, _, far, _, _ in self.ends():
                    if step == self.size - far:
                        skips.append(self.me == end)
            unless(skips, self.copy(c, step).wait_recv)
        total = self.part[c, self.me].astype(F32)
        for slot in range(self.size - 1):
            total = total + self.got[c, slot].astype(F32)
        return total

    def finish(self, chunks):
        for c in range(chunks):
            for step in range(1, self.size):
                self.copy(c, step).wait_send()


class LineGather:
    def __init__(self, name, size, group, mine, everyone, send, recv, relay_send):
        self.name, self.size, self.me = name, size, lax.axis_index(name)
        self.mine, self.everyone = mine, everyone
        self.send, self.recv, self.relay_send = send, recv, relay_send
        self.relays = size >= 3
        self.direct = [c for c in range(mine.shape[0]) if c % group >= group - DIRECT_LAST or (group > 2 and c >= 2 * group - 2)]

    def copy(self, c, step):
        peer = lax.rem(self.me + step, self.size)
        return remote(
            self.name, peer, self.mine.at[c], self.everyone.at[c, self.me],
            self.send.at[c, step - 1], self.recv.at[c, step - 1],
        )

    def skips(self, c, step):
        if not self.relays or c in self.direct:
            return []
        skips = []
        if step != self.size - 1:
            skips.append(self.me == self.size - step)
        if step != 1:
            skips.append(self.me == self.size - 1 - step)
        return skips

    def start(self, c):
        for step in order(self.size):
            unless(self.skips(c, step), self.copy(c, step).start)

    def forwards(self):
        last = self.size - 1
        return ((1, 0, range(2, self.size)), (last - 1, last, range(last - 2, -1, -1)))

    def onward(self, c, end, source):
        step = (end - source) % self.size
        block = self.everyone.at[c, source]
        return remote(
            self.name, end, block, block, self.relay_send.at[c, source], self.recv.at[c, step - 1]
        )

    def forward(self, c):
        if not self.relays or c in self.direct:
            return
        for neighbour, end, sources in self.forwards():

            @pl.when(self.me == neighbour)
            def _():
                for source in sources:
                    step = (neighbour - source) % self.size
                    self.copy(c, step).wait_recv()
                    self.onward(c, end, source).start()

    def wait(self, c):
        for step in order(self.size):
            skips = []
            if self.relays and c not in self.direct:
                if step != 1:
                    skips.append(self.me == 1)
                if step != self.size - 1:
                    skips.append(self.me == self.size - 2)
            unless(skips, self.copy(c, step).wait_recv)

    def finish(self, chunks):
        for c in range(chunks):
            for step in range(1, self.size):
                unless(self.skips(c, step), self.copy(c, step).wait_send)
            if self.relays and c not in self.direct:
                for neighbour, end, sources in self.forwards():

                    @pl.when(self.me == neighbour)
                    def _():
                        for source in sources:
                            self.onward(c, end, source).wait_send()


def silu(values):
    return values * jax.nn.sigmoid(values)


def softplus(values):
    return jnp.maximum(values, 0.0) + jnp.log1p(jnp.exp(-jnp.abs(values)))


def row_blocks(name, columns):
    return pl.ds(pl.multiple_of(lax.axis_index(name) * columns, LANES), columns)


def layer_kernel(
    n_kv, n_tp, width, head, repeat, chunks, pieces, halves,
    stream, lengths, gain, decay_log, time_bias, out_gain, mlp_gain,
    w_b, w_d, w_q, w_k, w_v, w_g, q_hist, k_hist, v_hist, conv_q, conv_k, conv_v,
    w_out, w_up, w_down, state,
    result, new_state,
    stream_v, len_v, gain_v, dlog_v, bias_v, ogain_v, mgain_v,
    wb_v, wd_v, wq_v, wk_v, wv_v, wg_v, hist_q, hist_k, hist_v, convq_v, convk_v, convv_v,
    wo_v, wu_v, wdn_v,
    gains, params, streams, part_e, got_e,
    part_p, got_p, relay_pi, relay_po,
    readouts,
    mine, gathered, mix_part, mix_got, mixed, blocks, sq_part, sq_got,
    up_part, up_got, relay_ui, relay_uo, hidden, hiddens, down_part, down_got,
    load_sem, state_sem, s_send, s_recv, e_send, e_recv,
    p_send, p_recv, p_relay, g_send, g_recv, g_relay,
    m_send, m_recv, b_send, b_recv, q_send, q_recv,
    u_send, u_recv, u_relay, h_send, h_recv, h_relay, d_send, d_recv,
):
    kv = lax.axis_index("kv")
    tp = lax.axis_index("tp")
    rows, own_cols = stream_v.shape
    own = rows // n_kv
    share = own // halves
    half_rows = n_kv * share
    block = wq_v.shape[0]
    heads_all = w_b.shape[0]
    heads_own = chunks * repeat
    span = repeat * head
    block_cols = row_blocks("kv", block)

    sources = (
        (stream, stream_v),
        (gain, gain_v),
        (w_b.at[:, block_cols], wb_v), (w_d.at[:, block_cols], wd_v),
        (w_q, wq_v), (w_k, wk_v), (w_v, wv_v), (w_g, wg_v),
        (lengths, len_v), (decay_log, dlog_v), (time_bias, bias_v),
        (out_gain, ogain_v), (mlp_gain, mgain_v),
        (q_hist, hist_q), (k_hist, hist_k), (v_hist, hist_v),
        (conv_q.at[:, row_blocks("tp", convq_v.shape[1])], convq_v),
        (conv_k.at[:, row_blocks("tp", convk_v.shape[1])], convk_v),
        (conv_v.at[:, row_blocks("tp", convv_v.shape[1])], convv_v),
        (w_out, wo_v), (w_up, wu_v), (w_down, wdn_v),
    )
    loads = [pltpu.make_async_copy(src, dst, load_sem.at[i]) for i, (src, dst) in enumerate(sources)]
    state_loads = [
        pltpu.make_async_copy(
            state.at[:, c * repeat : (c + 1) * repeat],
            new_state.at[:, c * repeat : (c + 1) * repeat],
            state_sem.at[c],
        )
        for c in range(chunks)
    ]
    start(loads[:19])
    start(state_loads)
    start(loads[19:])

    scatter_p = LineScatter("kv", n_kv, halves * chunks, part_p, got_p, relay_pi, relay_po, p_send, p_recv, p_relay)
    gather_g = LineGather("kv", n_kv, chunks, mine, gathered, g_send, g_recv, g_relay)
    scatter_u = LineScatter("kv", n_kv, pieces, up_part, up_got, relay_ui, relay_uo, u_send, u_recv, u_relay)
    gather_h = LineGather("kv", n_kv, pieces, hidden, hiddens, h_send, h_recv, h_relay)
    scatter_p.clear()
    scatter_u.clear()

    greet((("kv", n_kv), ("tp", n_tp)))
    loads[0].wait()
    stream_copies = gather_copies("tp", n_tp, stream_v, streams, s_send, s_recv)
    start(stream_copies)
    streams[tp] = stream_v[...]
    loads[1].wait()

    def gain_row(values):
        gains[...] = values[...].astype(F32)
        lines = block // LANES
        return jnp.concatenate(
            [gains[pl.ds(kv * lines + j, 1), :] for j in range(lines)], axis=1
        )

    norm_row = gain_row(gain_v)
    wait_recv(stream_copies)

    wide = jnp.concatenate([streams[t] for t in range(n_tp)], axis=1).astype(F32)
    scaled = (wide * norm_row).astype(BF16)

    def extras():
        loads[2].wait()
        loads[3].wait()
        beta = lax.dot_general(scaled, wb_v[...], CONTRACT_LAST, preferred_element_type=F32)
        decay = lax.dot_general(scaled, wd_v[...], CONTRACT_LAST, preferred_element_type=F32)
        squares = jnp.sum(wide * wide, axis=1, keepdims=True)
        coarse = squares.astype(BF16)
        fine = (squares - coarse.astype(F32)).astype(BF16)
        spare = (LANES - 2 * heads_all) // 2
        part_e[...] = jnp.concatenate(
            [
                beta.astype(BF16), decay.astype(BF16),
                jnp.broadcast_to(coarse, (rows, spare)), jnp.broadcast_to(fine, (rows, spare)),
            ],
            axis=1,
        ).reshape(n_kv, own, LANES)
        copies = scatter_copies("kv", n_kv, part_e, got_e, e_send, e_recv)
        start(copies)
        return copies

    for copy in loads[4:8]:
        copy.wait()
    fields = ((wq_v, head, 0), (wk_v, head, head), (wv_v, span, 2 * head), (wg_v, span, 2 * head + span))
    for c in range(chunks):
        for weight, size, offset in fields:
            product = jnp.dot(
                scaled, weight[:, c * size : (c + 1) * size], preferred_element_type=F32
            )
            split = product.reshape(n_kv, own, size).astype(BF16)
            for h in range(halves):
                part_p[h * chunks + c, :, :, offset : offset + size] = split[
                    :, h * share : (h + 1) * share
                ]
        scatter_p.start(c)
        if c == 0:
            extra_copies = extras()

    for copy in loads[8:19]:
        copy.wait()
    lens_row = jnp.broadcast_to(len_v[...].astype(F32), (own, own))
    diagonal = lax.broadcasted_iota(jnp.int32, (own, own), 0) == lax.broadcasted_iota(
        jnp.int32, (own, own), 1
    )
    length = jnp.sum(jnp.where(diagonal, lens_row, 0.0), axis=1, keepdims=True)

    def history(hist, taps):
        total = None
        count = taps.shape[0]
        for r in range(count - 1):
            live = length >= float(count - r)
            term = jnp.where(live, hist[r].astype(F32) * taps[r : r + 1, :], 0.0)
            total = term if total is None else total + term
        return total

    taps_q = convq_v[...].astype(F32)
    taps_k = convk_v[...].astype(F32)
    taps_v = convv_v[...].astype(F32)
    past_q = history(hist_q, taps_q)
    past_k = history(hist_k, taps_k)
    past_v = history(hist_v, taps_v)
    final = taps_q.shape[0] - 1

    params[...] = jnp.zeros(params.shape, F32)
    params[0:1, :heads_all] = dlog_v[...]
    params[1:2, :heads_all] = bias_v[...]
    shift = tp * heads_own
    own_params = pltpu.roll(params[...], lax.rem(LANES - shift, LANES), 1)

    scatter_p.relay(0)
    wait_recv(extra_copies)
    extra = part_e[kv].astype(F32)
    for slot in range(n_kv - 1):
        extra = extra + got_e[slot].astype(F32)
    fine_at = heads_all + LANES // 2
    square_sum = extra[:, 2 * heads_all : 2 * heads_all + 1] + extra[:, fine_at : fine_at + 1]
    row_scale = lax.rsqrt(square_sum / width + EPSILON)
    terms = extra * row_scale
    own_beta = pltpu.roll(terms, lax.rem(LANES - shift, LANES), 1)
    own_decay = pltpu.roll(terms, lax.rem(2 * LANES - heads_all - shift, LANES), 1)
    fade = jnp.exp(-jnp.exp(own_params[0:1, :]) * softplus(own_decay + own_params[1:2, :]))
    fade = jnp.where(length == 1.0, 0.0, fade)
    strength = jax.nn.sigmoid(own_beta)
    gain_out = ogain_v[...].astype(F32)

    def unit(values, factor):
        return values * (
            lax.rsqrt(jnp.sum(values * values, axis=1, keepdims=True) + EPSILON) * factor
        )

    seqs = readouts.shape[1]

    def heads(h, c):
        index = h * chunks + c
        these = slice(h * share, (h + 1) * share)
        total = scatter_p.total(index) * row_scale[these]
        narrow = slice(c * head, (c + 1) * head)
        broad = slice(c * span, (c + 1) * span)
        query = unit(
            silu(total[:, :head] * taps_q[final : final + 1, narrow] + past_q[these, narrow]),
            head ** (-0.5),
        )
        key = unit(
            silu(total[:, head : 2 * head] * taps_k[final : final + 1, narrow] + past_k[these, narrow]),
            1.0,
        )
        values = silu(
            total[:, 2 * head : 2 * head + span] * taps_v[final : final + 1, broad] + past_v[these, broad]
        )
        gate = silu(total[:, 2 * head + span :])
        dot = jnp.sum(query * key, axis=1, keepdims=True)
        owned = range(c * repeat, (c + 1) * repeat)

        def widen(columns):
            return jnp.concatenate(
                [jnp.broadcast_to(column, (share, head)) for column in columns], axis=1
            )

        dots = widen([dot] * repeat)
        fades = widen([fade[these, v : v + 1] for v in owned])
        strengths = widen([strength[these, v : v + 1] for v in owned])
        keys_t = key.T
        line = lax.broadcasted_iota(jnp.int32, (seqs, span), 0)
        if h == 0:
            state_loads[c].wait()

        def ask(g):
            some = slice(g * seqs, (g + 1) * seqs)
            both = jnp.concatenate([key[some], query[some]], axis=0).astype(BF16)
            recalled = jnp.zeros((seqs, span), F32)
            asked = jnp.zeros((seqs, span), F32)
            for s in range(seqs):
                q = h * share + g * seqs + s
                held = jnp.concatenate([new_state[q, v] for v in owned], axis=1)
                answer = jnp.dot(both, held.astype(BF16), preferred_element_type=F32)
                recalled = jnp.where(line == s, answer[:seqs], recalled)
                asked = jnp.where(line == s, answer[seqs:], asked)
            faded = fades[some]
            update = strengths[some] * (values[some] - faded * recalled)
            readouts[g] = faded * asked + dots[some] * update
            return faded, update

        def apply(g, faded, update):
            for s in range(seqs):
                q = h * share + g * seqs + s
                near = g * seqs + s
                wide_key = jnp.broadcast_to(keys_t[:, near : near + 1], (head, head))
                for j, v in enumerate(owned):
                    cols = slice(j * head, (j + 1) * head)
                    new_state[q, v] = (
                        new_state[q, v] * faded[s : s + 1, cols] + wide_key * update[s : s + 1, cols]
                    )

        groups = share // seqs
        ready = ask(0)
        for g in range(groups):
            later = ask(g + 1) if g + 1 < groups else None
            apply(g, *ready)
            ready = later

        for j in range(repeat):
            cols = slice(j * head, (j + 1) * head)
            one = readouts[:, :, cols].reshape(share, head)
            normed = one * lax.rsqrt(jnp.mean(one * one, axis=1, keepdims=True) + EPSILON)
            mine[index, :, cols] = (normed * gain_out * gate[:, cols]).astype(BF16)
        gather_g.start(index)
        gathered[index, kv] = mine[index]

    def project_relay(h, c):
        scatter_p.relay(h * chunks + c)

    def project_start(h, c):
        scatter_p.start(h * chunks + c)

    def gated_forward(h, c):
        gather_g.forward(h * chunks + c)

    copies_of = {}

    def send_tp(name, h, product, part, got, send_sem, recv_sem):
        for t in range(n_tp):
            part[h, t] = product[:, t * own_cols : (t + 1) * own_cols].astype(BF16)
        copies = scatter_copies("tp", n_tp, part.at[h], got.at[h], send_sem.at[h], recv_sem.at[h])
        start(copies)
        copies_of[name, h] = copies

    def sum_tp(name, h, part, got):
        wait_recv(copies_of[name, h])
        total = part[h, tp].astype(F32)
        for slot in range(n_tp - 1):
            total = total + got[h, slot].astype(F32)
        return total

    def out_project(h):
        if h == 0:
            loads[19].wait()
        product = jnp.zeros((half_rows, wo_v.shape[1]), F32)
        for c in range(chunks):
            gather_g.wait(h * chunks + c)
            product = product + jnp.dot(
                gathered[h * chunks + c].reshape(half_rows, span),
                wo_v[c * span : (c + 1) * span, :],
                preferred_element_type=F32,
            )
        send_tp("mix", h, product, mix_part, mix_got, m_send, m_recv)

    def mix(h):
        total = sum_tp("mix", h, mix_part, mix_got)
        before = jnp.concatenate(
            [stream_v[z * own + h * share : z * own + (h + 1) * share, :] for z in range(n_kv)], axis=0
        )
        mixed_own = (before.astype(F32) + total).astype(BF16)
        mixed[h] = mixed_own
        copies = gather_copies("tp", n_tp, mixed.at[h], blocks.at[h], b_send.at[h], b_recv.at[h])
        start(copies)
        copies_of["block", h] = copies
        blocks[h, tp] = mixed_own

    mlp_row = gain_row(mgain_v)
    piece = wu_v.shape[1] // pieces
    corner = lax.broadcasted_iota(jnp.int32, (half_rows, half_rows), 0) == lax.broadcasted_iota(
        jnp.int32, (half_rows, half_rows), 1
    )

    def up(h):
        if h == 0:
            loads[20].wait()
        wait_recv(copies_of["block", h])
        wide = jnp.concatenate([blocks[h, t] for t in range(n_tp)], axis=1).astype(F32)
        scaled = (wide * mlp_row).astype(BF16)
        for p in range(pieces):
            product = jnp.dot(
                scaled, wu_v[:, p * piece : (p + 1) * piece], preferred_element_type=F32
            )
            up_part[h * pieces + p] = product.reshape(n_kv, share, piece).astype(BF16)
            scatter_u.start(h * pieces + p)
        squares = jnp.sum(wide * wide, axis=1, keepdims=True)
        flat = jnp.sum(jnp.where(corner, squares, 0.0), axis=0, keepdims=True)
        sq_part[h, :, :half_rows] = jnp.broadcast_to(flat, (sq_part.shape[1], half_rows))
        copies = gather_copies("kv", n_kv, sq_part.at[h], sq_got.at[h], q_send.at[h], q_recv.at[h])
        start(copies)
        copies_of["square", h] = copies
        sq_got[h, kv, :, :half_rows] = sq_part[h, :, :half_rows]

    def up_relay(h, p):
        scatter_u.relay(h * pieces + p)

    def activate(h, p):
        index = h * pieces + p
        active = jnp.maximum(scatter_u.total(index), 0.0)
        active = (active * active).astype(BF16)
        hidden[index] = active
        gather_h.start(index)
        hiddens[index, kv] = active

    def hidden_forward(h, p):
        gather_h.forward(h * pieces + p)

    def down(h):
        if h == 0:
            loads[21].wait()
        wait_recv(copies_of["square", h])
        square_sum = sq_got[h, 0, :, :half_rows]
        for z in range(1, n_kv):
            square_sum = square_sum + sq_got[h, z, :, :half_rows]
        spread = jnp.broadcast_to(
            1.0 / (square_sum[0:1, :] / width + EPSILON), (half_rows, half_rows)
        )
        scale_squared = jnp.sum(jnp.where(corner, spread, 0.0), axis=1, keepdims=True)
        product = jnp.zeros((half_rows, wdn_v.shape[1]), F32)
        for p in range(pieces):
            index = h * pieces + p
            gather_h.wait(index)
            product = product + jnp.dot(
                hiddens[index].reshape(half_rows, piece),
                wdn_v[p * piece : (p + 1) * piece, :],
                preferred_element_type=F32,
            )
        send_tp("down", h, product * scale_squared, down_part, down_got, d_send, d_recv)

    def finish(h):
        total = sum_tp("down", h, down_part, down_got)
        ended = (mixed[h].astype(F32) + total).astype(BF16)
        for z in range(n_kv):
            result[z * own + h * share : z * own + (h + 1) * share, :] = ended[
                z * share : (z + 1) * share
            ]

    def settle_projections():
        wait_send(stream_copies)
        wait_send(extra_copies)
        scatter_p.finish(halves * chunks)
        gather_g.finish(halves * chunks)

    def settle_hidden():
        for name in ("mix", "block", "square"):
            for h in range(halves):
                wait_send(copies_of[name, h])
        scatter_u.finish(halves * pieces)
        gather_h.finish(halves * pieces)

    last = chunks - 1
    for c in range(chunks):
        if c < last:
            project_relay(0, c + 1)
        heads(0, c)
        if halves > 1:
            project_start(1, c)
    if halves == 1:
        for c in range(chunks):
            gated_forward(0, c)
        out_project(0)
        mix(0)
        settle_projections()
        up(0)
        for p in range(pieces):
            up_relay(0, p)
            activate(0, p)
        for p in range(pieces):
            hidden_forward(0, p)
        down(0)
    else:
        project_relay(1, 0)
        gated_forward(0, 0)
        for c in range(chunks):
            if c < last:
                project_relay(1, c + 1)
            heads(1, c)
            if c + 1 < last:
                gated_forward(0, c + 1)
            if c == last - 1:
                gated_forward(0, last)
                out_project(0)
        gated_forward(1, 0)
        mix(0)
        for c in range(1, chunks):
            gated_forward(1, c)
        out_project(1)
        settle_projections()
        up(0)
        mix(1)
        up_relay(0, 0)
        up(1)
        for p in range(1, pieces):
            up_relay(0, p)
        for p in range(pieces):
            activate(0, p)
            up_relay(1, p)
        for p in range(pieces):
            hidden_forward(0, p)
        for p in range(pieces):
            activate(1, p)
        down(0)
        for p in range(pieces):
            hidden_forward(1, p)
        finish(0)
        down(1)
    settle_hidden()
    finish(halves - 1)
    for h in range(halves):
        wait_send(copies_of["down", h])


def store_kernel(result_v, state_v, result, state, sems):
    parts = sems.shape[0] - 1
    each = state_v.shape[0] // parts
    copies = [
        pltpu.make_async_copy(
            state_v.at[i * each : (i + 1) * each], state.at[i * each : (i + 1) * each], sems.at[i]
        )
        for i in range(parts)
    ]
    copies.append(pltpu.make_async_copy(result_v, result, sems.at[parts]))
    start(copies)
    for copy in copies:
        copy.wait()


def on_device(
    n_kv, n_tp,
    stream, lengths, delta_state, q_hist, k_hist, v_hist, norm_gain,
    w_query, w_key, w_value, w_gate, w_beta, w_decay,
    conv_query, conv_key, conv_value, decay_log, time_bias, out_gain,
    w_out, mlp_gain, w_up, w_down,
):
    width = norm_gain.shape[0]
    rows, own_cols = stream.shape
    own, heads_own, head = delta_state.shape[:3]
    key_cols = q_hist.shape[2]
    value_cols = v_hist.shape[2]
    block = w_query.shape[0]
    heads_all = w_beta.shape[1]
    taps = conv_query.shape[0]
    chunks = key_cols // head
    repeat = heads_own // chunks
    span = repeat * head
    field = 2 * head + 2 * span
    units = w_up.shape[1]
    seqs = min(8, own)
    halves = 2 if own % (4 * seqs) == 0 else 1
    share = own // halves
    half_rows = n_kv * share
    pieces = 4 // halves
    piece = units // pieces
    ids = halves * chunks
    shares = halves * pieces
    vmem = pl.BlockSpec(memory_space=pltpu.VMEM)
    hbm = pl.BlockSpec(memory_space=pltpu.HBM)
    dma = pltpu.SemaphoreType.DMA
    gain_shape = (width // LANES, LANES)
    ins = (
        stream, lengths[None], norm_gain.reshape(gain_shape), decay_log[None], time_bias[None],
        out_gain[None], mlp_gain.reshape(gain_shape),
        w_beta.T, w_decay.T, w_query, w_key, w_value, w_gate,
        *(jnp.transpose(hist, (1, 0, 2)) for hist in (q_hist, k_hist, v_hist)),
        conv_query, conv_key, conv_value, w_out, w_up, w_down, delta_state,
    )

    def buffer(*dims, dtype=BF16):
        return pltpu.VMEM(dims, dtype)

    result, new_state = pl.pallas_call(
        functools.partial(layer_kernel, n_kv, n_tp, width, head, repeat, chunks, pieces, halves),
        out_shape=(
            pltpu.VMEM((rows, own_cols), BF16),
            pltpu.VMEM(delta_state.shape, F32),
        ),
        in_specs=[hbm] * len(ins),
        out_specs=(vmem, vmem),
        scratch_shapes=[
            buffer(rows, own_cols), buffer(1, own, dtype=jnp.int32), buffer(*gain_shape),
            buffer(1, heads_all, dtype=F32), buffer(1, heads_all, dtype=F32),
            buffer(1, head), buffer(*gain_shape),
            buffer(heads_all, block), buffer(heads_all, block),
            buffer(block, key_cols), buffer(block, key_cols),
            buffer(block, value_cols), buffer(block, value_cols),
            buffer(taps - 1, own, key_cols), buffer(taps - 1, own, key_cols),
            buffer(taps - 1, own, value_cols),
            buffer(taps, key_cols), buffer(taps, key_cols), buffer(taps, value_cols),
            buffer(*w_out.shape), buffer(*w_up.shape), buffer(*w_down.shape),
            buffer(*gain_shape, dtype=F32), buffer(8, LANES, dtype=F32),
            buffer(n_tp, rows, own_cols),
            buffer(n_kv, own, LANES), buffer(n_kv - 1, own, LANES),
            buffer(ids, n_kv, share, field), buffer(ids, n_kv - 1, share, field),
            buffer(ids, share, field), buffer(ids, share, field),
            buffer(share // seqs, seqs, span, dtype=F32),
            buffer(ids, share, span), buffer(ids, n_kv, share, span),
            buffer(halves, n_tp, half_rows, own_cols), buffer(halves, n_tp - 1, half_rows, own_cols),
            buffer(halves, half_rows, own_cols), buffer(halves, n_tp, half_rows, own_cols),
            buffer(halves, 8, rows, dtype=F32), buffer(halves, n_kv, 8, rows, dtype=F32),
            buffer(shares, n_kv, share, piece), buffer(shares, n_kv - 1, share, piece),
            buffer(shares, share, piece), buffer(shares, share, piece),
            buffer(shares, share, piece), buffer(shares, n_kv, share, piece),
            buffer(halves, n_tp, half_rows, own_cols), buffer(halves, n_tp - 1, half_rows, own_cols),
            dma((22,)), dma((chunks,)),
            dma((n_tp - 1,)), dma((n_tp - 1,)),
            dma((n_kv - 1,)), dma((n_kv - 1,)),
            dma((ids, n_kv - 1)), dma((ids, n_kv - 1)), dma((ids,)),
            dma((ids, n_kv - 1)), dma((ids, n_kv - 1)), dma((ids, n_kv)),
            dma((halves, n_tp - 1)), dma((halves, n_tp - 1)),
            dma((halves, n_tp - 1)), dma((halves, n_tp - 1)),
            dma((halves, n_kv - 1)), dma((halves, n_kv - 1)),
            dma((shares, n_kv - 1)), dma((shares, n_kv - 1)), dma((shares,)),
            dma((shares, n_kv - 1)), dma((shares, n_kv - 1)), dma((shares, n_kv)),
            dma((halves, n_tp - 1)), dma((halves, n_tp - 1)),
        ],
        compiler_params=pltpu.CompilerParams(
            collective_id=0, has_side_effects=True,
            vmem_limit_bytes=67043328 - delta_state.size * 4 - 2**18,
        ),
        name="layer",
    )(*ins)
    return pl.pallas_call(
        store_kernel,
        out_shape=(
            jax.ShapeDtypeStruct(result.shape, BF16),
            jax.ShapeDtypeStruct(delta_state.shape, F32),
        ),
        in_specs=[vmem, vmem],
        out_specs=(hbm, hbm),
        scratch_shapes=[dma((min(own, 8) + 1,))],
        compiler_params=pltpu.CompilerParams(vmem_limit_bytes=2**20),
        name="store",
    )(result, new_state)


def solution(mesh):
    in_specs = (
        P("grp", ("kv", "tp")),
        P(("grp", "kv")),
        P(("grp", "kv"), "tp", None, None),
        P(("grp", "kv"), None, "tp"),
        P(("grp", "kv"), None, "tp"),
        P(("grp", "kv"), None, "tp"),
        P(),
        P("kv", "tp"),
        P("kv", "tp"),
        P("kv", "tp"),
        P("kv", "tp"),
        P(),
        P(),
        P(),
        P(),
        P(),
        P(),
        P(),
        P(),
        P("tp", "kv"),
        P(),
        P("kv", "tp"),
        P("tp", "kv"),
    )
    out_specs = (P("grp", ("kv", "tp")), P(("grp", "kv"), "tp", None, None))
    return jax.shard_map(
        functools.partial(on_device, mesh.shape["kv"], mesh.shape["tp"]),
        mesh=mesh, in_specs=in_specs, out_specs=out_specs, check_vma=False,
    )
```
